32 devices in a mesh: sp: 8 (over z, core), tp: 4 (over y, x).
Axes of the slice: x: 2, y: 2, z: 4, core: 2. Of those that a mesh axis runs over, the one named last changes fastest.
Arguments:
- residual: bfloat16 [1024, 2048], P('sp', 'tp'), may hold values from -48 to 48
- glu_value: bfloat16 [1024, 2048], P('sp', 'tp'), may hold values from -48 to 48
- glu_gate: bfloat16 [1024, 2048], P('sp', 'tp'), may hold values from -6 to 6
- conv_weight: bfloat16 [31, 2048], P(None, 'tp'), may hold values from -1 to 1
- conv_bias: float32 [2048], P('tp'), may hold values from -3 to 3
- ln_gain: float32 [2048], P('tp'), may hold values from 0.1 to 1.9
- ln_bias: float32 [2048], P('tp'), may hold values from -3 to 3
- out_weight: bfloat16 [2048, 2048], P(None, 'tp'), may hold values from -0.125 to 0.125
- norm_gain: float32 [2048], P('tp'), may hold values from 0.1 to 1.9
- route_ids: int32 [1024, 2], P('sp'), may hold values from 0 to 7, all different within a row; in each aligned block of 128 rows (0 to 127, 128 to 255, ...) at most 64 rows name the same one
- route_weight: float32 [1024, 2], P('sp'), may hold values from 0.1 to 1
- expert_gate: bfloat16 [8, 2048, 4096], P('sp', None, 'tp'), may hold values from -0.125 to 0.125
- expert_up: bfloat16 [8, 2048, 4096], P('sp', None, 'tp'), may hold values from -0.125 to 0.125
- expert_down: bfloat16 [8, 4096, 2048], P('sp', 'tp'), may hold values from -0.09375 to 0.09375
Outputs:
- layer_out: bfloat16 [1024, 2048], P('sp', 'tp')
The draws below stay inside these ranges and needn't reach their ends.
Inputs may be any that keep to these rules, and one draw needn't show every extreme that they name: `route_ids`: within the 128 rows of one index of sp, no expert is named more than 64 times, and in some such rows one expert is named exactly 64 times.
All inputs are finite; a program needn't handle non-finite values.
Results may differ from the reference program's by a relative error of at most 0.006.
Values may be sent and summed in bfloat16 or wider, within the bound.
A program may use at most 64 MiB of HBM per device.

```python
import math
import jax
import jax.numpy as jnp
import numpy as np
from jax import lax

D = 2048
FF = 4096
KERNEL = 31
TOPK = 2
ROWS = 128
TOKENS = 1024
EXPERTS = 8
CAP = 64
N_SP = 8
N_TP = 4


def rising_field(key, low, high):
    ramp = jnp.exp(jnp.linspace(math.log(low), math.log(high), D)).astype(jnp.float32)
    base = jnp.clip(jax.random.normal(key, (TOKENS, D), jnp.float32), -6.0, 6.0)
    return base * ramp


def draw_residual(key, part):
    return rising_field(jax.random.fold_in(key, 11), 0.5, 2.0).astype(jnp.bfloat16)


def draw_glu_value(key, part):
    return rising_field(jax.random.fold_in(key, 23), 0.5, 2.0).astype(jnp.bfloat16)


def levels(stream_key, dims, shards, least, largest):
    def one(position, parts):
        heights = jax.random.uniform(jax.random.fold_in(jax.random.fold_in(stream_key, 6), position), (parts,), jnp.float32, least / len(shards), largest / len(shards))
        return jnp.repeat(jnp.exp(heights), dims[position] // parts).reshape((-1,) + (1,) * (len(dims) - position - 1))

    loudness = one(*shards[0])
    for cut in shards[1:]:
        loudness = loudness * one(*cut)
    return loudness


def routed_block(rng, own, number, rows, count, top, most, skew):
    order = jax.random.permutation(rng, count)
    heavy_load, ordinary = portions_of(count, rows * top, most, skew, True), portions_of(count, rows * top, most, skew, False)
    places = jnp.arange(count)

    def named(lengths, turn):
        used = int((lengths > 0).sum())
        fixed = max(1, used // 4)
        moved = fixed + (places - fixed + turn * (used - fixed)) % max(1, count - fixed)
        return jnp.zeros((count,), jnp.int32).at[order[jnp.where(places < fixed, places, moved)]].set(jnp.asarray(lengths, jnp.int32))

    lengths = jnp.where(number % 4 == 0, named(heavy_load, number // 4), named(ordinary, number - number // 4 - 1))
    mixed = jax.random.permutation(jax.random.fold_in(own, 3), count)
    giver, sink = mixed[0:count // 2 * 2:2], mixed[1:count // 2 * 2:2]
    slack = jnp.minimum(lengths[giver] - 1, most - lengths[sink]) // 2
    slack = jnp.where((giver == order[0]) | (sink == order[0]) | (lengths[sink] == 0), 0, jnp.maximum(slack, 0))
    moved = jax.random.randint(jax.random.fold_in(own, 4), (count // 2,), 0, 1 << 20) % (slack + 1)
    lengths = lengths.at[giver].add(-moved).at[sink].add(moved)
    items = jnp.searchsorted(jnp.cumsum(lengths), jnp.arange(rows * top), side="right").astype(jnp.int32)
    table = items.reshape(top, rows).T
    table = table[jax.random.permutation(jax.random.fold_in(own, 1), rows)]
    turn = jax.random.randint(jax.random.fold_in(own, 2), (rows, 1), 0, top)
    return jnp.take_along_axis(table, (jnp.arange(top)[None, :] + turn) % top, axis=1)


def portions_of(count, total, bound, lean, full):
    loads = [(1 << 20) // math.isqrt(rank ** lean) + 1 for rank in range(1, count + 1)]
    largest = bound if full else min(bound, max(-(-total // count), total * loads[0] // sum(loads)))
    least = 1 if total - largest >= count - 1 else 0
    counts, spare = [largest] + [least] * (count - 1), total - largest - least * (count - 1)
    while spare > 0:
        candidates = [i for i in range(1, count) if counts[i] < largest] or [i for i in range(1, count) if counts[i] < bound]
        whole, left = sum([loads[i] for i in candidates]), spare
        for i in candidates:
            extra = min(bound - counts[i], max(1, left * loads[i] // whole), spare)
            counts[i] = counts[i] + extra
            spare = spare - extra
    return np.array(counts)


def gaussian(rng, shape, spread, limit, cuts=(), kind=jnp.bfloat16):
    drawn = spread * jax.random.normal(rng, shape, jnp.float32)
    if cuts:
        drawn = drawn * levels(rng, shape, cuts, -0.22, 0.18)
    return jnp.clip(drawn, -limit, limit).astype(kind)


def setup_inputs(seed: int = 0) -> dict:
    arg_keys = jax.random.split(jax.random.key(seed), 15)
    residual = draw_residual(jax.random.fold_in(arg_keys[14], 71), 0)
    glu_value = draw_glu_value(jax.random.fold_in(arg_keys[14], 71), 0)
    glu_gate = gaussian(arg_keys[2], (TOKENS, D), 1.0, 6.0, ((0, 8), (1, 4)))
    conv_weight = gaussian(arg_keys[3], (KERNEL, D), KERNEL ** -0.5, 1.0, ((1, 4),))
    conv_bias = gaussian(arg_keys[4], (D,), 0.5, 3.0, ((0, 4),), jnp.float32)
    ln_gain = jnp.clip(1.0 + 0.18 * jax.random.normal(arg_keys[5], (D,), jnp.float32), 0.1, 1.9)
    ln_bias = gaussian(arg_keys[6], (D,), 0.5, 3.0, ((0, 4),), jnp.float32)
    out_weight = gaussian(arg_keys[7], (D, D), D ** -0.5, 0.125, ((1, 4),))
    norm_gain = jnp.clip(1.0 + 0.18 * jax.random.normal(arg_keys[8], (D,), jnp.float32), 0.1, 1.9)
    route_ids_keys = jax.random.split(jax.random.fold_in(arg_keys[9], 1), TOKENS // ROWS)
    route_ids_turns = jax.random.permutation(jax.random.fold_in(arg_keys[9], 3), TOKENS // ROWS)
    route_ids = jax.vmap(lambda own, number: routed_block(jax.random.fold_in(arg_keys[9], 2), own, number, ROWS, EXPERTS, TOPK, CAP, 2))(route_ids_keys, route_ids_turns).reshape((TOKENS, TOPK))
    route_weight = jnp.clip(jnp.exp(math.log(1.0) - 2.3025851 * jax.random.uniform(arg_keys[10], (TOKENS, TOPK), jnp.float32) ** levels(arg_keys[10], (TOKENS, TOPK), ((0, 8),), -0.2, 0.2)), 0.1, 1.0)
    expert_gate = gaussian(arg_keys[11], (EXPERTS, D, FF), D ** -0.5, 0.125, ((0, 8), (2, 4)))
    expert_up = gaussian(arg_keys[12], (EXPERTS, D, FF), D ** -0.5, 0.125, ((0, 8), (2, 4)))
    expert_down = gaussian(arg_keys[13], (EXPERTS, FF, D), FF ** -0.5, 0.09375, ((0, 8), (1, 4)))
    return dict(residual=residual, glu_value=glu_value, glu_gate=glu_gate, conv_weight=conv_weight, conv_bias=conv_bias, ln_gain=ln_gain, ln_bias=ln_bias, out_weight=out_weight, norm_gain=norm_gain, route_ids=route_ids, route_weight=route_weight, expert_gate=expert_gate, expert_up=expert_up, expert_down=expert_down)


def reference(residual, glu_value, glu_gate, conv_weight, conv_bias, ln_gain, ln_bias, out_weight, norm_gain, route_ids, route_weight, expert_gate, expert_up, expert_down):
    gated = (glu_value.astype(jnp.float32) * jax.nn.sigmoid(glu_gate.astype(jnp.float32))).astype(jnp.bfloat16)
    reach = KERNEL // 2
    padded = jnp.pad(gated.astype(jnp.float32), ((reach, reach), (0, 0)))
    taps = conv_weight.astype(jnp.float32)
    conv = jnp.zeros(gated.shape, jnp.float32) + conv_bias
    for tap in range(KERNEL):
        conv = conv + padded[tap:tap + TOKENS] * taps[tap]
    mean = lax.optimization_barrier(jnp.mean(conv, axis=1, keepdims=True))
    var = lax.optimization_barrier(jnp.mean(conv * conv, axis=1, keepdims=True)) - mean * mean
    act = jax.nn.silu((conv - mean) * lax.rsqrt(var + 1e-05) * ln_gain + ln_bias).astype(jnp.bfloat16)
    mixed = residual.astype(jnp.float32) + jnp.dot(act, out_weight, preferred_element_type=jnp.float32)
    squares = lax.optimization_barrier(jnp.mean(mixed * mixed, axis=1, keepdims=True))
    normed = (mixed * lax.rsqrt(squares + 1e-06) * norm_gain).astype(jnp.bfloat16)
    flat = route_ids.reshape(-1)
    owner = (jnp.arange(TOKENS * TOPK, dtype=jnp.int32) // TOPK).astype(jnp.int32)
    weights = route_weight.reshape(-1)
    slots = N_SP * CAP
    slot_index = jnp.arange(slots, dtype=jnp.int32)
    block = FF // N_TP

    def per_expert(total, expert):
        chosen = flat == expert
        picks = jnp.nonzero(chosen, size=slots, fill_value=0)[0].astype(jnp.int32)
        count = jnp.sum(chosen.astype(jnp.int32))
        live = (slot_index < count).astype(jnp.float32)
        rows = normed[owner[picks]]
        gate = jnp.dot(rows, expert_gate[expert], preferred_element_type=jnp.float32)
        up = jnp.dot(rows, expert_up[expert], preferred_element_type=jnp.float32)
        hidden = (jax.nn.silu(gate) * up).astype(jnp.bfloat16)
        down = expert_down[expert]
        result = jnp.zeros((slots, D), jnp.float32)
        for part_index in range(N_TP):
            piece = jnp.dot(hidden[:, part_index * block:(part_index + 1) * block], down[part_index * block:(part_index + 1) * block], preferred_element_type=jnp.float32)
            result = result + piece.astype(jnp.bfloat16).astype(jnp.float32)
        result = result.astype(jnp.bfloat16)
        scaled = result.astype(jnp.float32) * (weights[picks] * live)[:, None]
        return (total.at[owner[picks]].add(scaled), None)
    moe, _ = lax.scan(per_expert, jnp.zeros((TOKENS, D), jnp.float32), jnp.arange(EXPERTS, dtype=jnp.int32))
    return (mixed + moe).astype(jnp.bfloat16)
```

```python
import functools

import jax
import jax.numpy as jnp
from jax import lax
from jax.experimental import pallas as pl
from jax.experimental.pallas import tpu as pltpu
from jax.sharding import PartitionSpec as P

TOPK = 2


def with_halo(cells, sides, width):
    for axis, dim in sides:
        count = lax.axis_size(axis)
        ends = count - 1
        head = lax.slice_in_dim(cells, 0, width, axis=dim)
        tail = lax.slice_in_dim(cells, cells.shape[dim] - width, cells.shape[dim], axis=dim)
        cells = jnp.concatenate(
            [
                lax.ppermute(tail, axis, [(i, (i + 1) % count) for i in range(ends)]),
                cells,
                lax.ppermute(head, axis, [((i + 1) % count, i) for i in range(ends)]),
            ],
            axis=dim,
        )
    return cells


def on_device(
    residual,
    glu_value,
    glu_gate,
    conv_weight,
    conv_bias,
    ln_gain,
    ln_bias,
    out_weight,
    norm_gain,
    route_ids,
    route_weight,
    expert_gate,
    expert_up,
    expert_down,
):
    rows = residual.shape[0]
    width_all = out_weight.shape[0]
    gated = (glu_value.astype(jnp.float32) * jax.nn.sigmoid(glu_gate.astype(jnp.float32))).astype(
        jnp.bfloat16
    )
    reach = conv_weight.shape[0] // 2
    padded = with_halo(gated, (("sp", 0),), reach)
    taps = conv_weight.astype(jnp.float32)
    conv = jnp.zeros(gated.shape, jnp.float32) + conv_bias
    for tap in range(conv_weight.shape[0]):
        conv = conv + padded[tap : tap + rows].astype(jnp.float32) * taps[tap]
    totals = lax.psum((jnp.sum(conv, axis=1), jnp.sum(conv * conv, axis=1)), "tp")
    mean = (totals[0] / width_all)[:, None]
    var = (totals[1] / width_all)[:, None] - mean * mean
    act = jax.nn.silu((conv - mean) * lax.rsqrt(var + 1e-05) * ln_gain + ln_bias).astype(
        jnp.bfloat16
    )
    projected = jnp.dot(
        lax.all_gather(act, "tp", axis=1, tiled=True),
        out_weight,
        preferred_element_type=jnp.float32,
    )
    mixed = residual.astype(jnp.float32) + projected
    squares = lax.psum(jnp.sum(mixed * mixed, axis=1), "tp")
    normed = (mixed * lax.rsqrt(squares / width_all + 1e-06)[:, None] * norm_gain).astype(
        jnp.bfloat16
    )
    experts = lax.axis_size("sp")
    capacity = 2 * rows * TOPK // experts
    flat = route_ids.reshape(-1)
    onehot = (flat[:, None] == jnp.arange(experts, dtype=jnp.int32)[None, :]).astype(jnp.int32)
    rank = jnp.sum((jnp.cumsum(onehot, axis=0) - 1) * onehot, axis=1)
    slot_of = flat * capacity + rank
    placing = (slot_of[None, :] == jnp.arange(experts * capacity, dtype=jnp.int32)[:, None]).astype(
        jnp.bfloat16
    )
    copies = jnp.repeat(normed, TOPK, axis=0)
    outgoing = jnp.dot(placing, copies, preferred_element_type=jnp.float32).astype(jnp.bfloat16)
    outgoing = outgoing.reshape(experts, capacity, normed.shape[1])
    arrived = lax.all_to_all(outgoing, "sp", split_axis=0, concat_axis=0, tiled=True)
    arrived = lax.all_gather(
        arrived.reshape(experts * capacity, normed.shape[1]), "tp", axis=1, tiled=True
    )
    gate = jnp.dot(arrived, expert_gate[0], preferred_element_type=jnp.float32)
    up = jnp.dot(arrived, expert_up[0], preferred_element_type=jnp.float32)
    hidden = (jax.nn.silu(gate) * up).astype(jnp.bfloat16)
    partial_out = jnp.dot(hidden, expert_down[0], preferred_element_type=jnp.float32)
    summed = lax.psum_scatter(
        partial_out.astype(jnp.bfloat16), "tp", scatter_dimension=1, tiled=True
    )
    summed = summed.reshape(experts, capacity, summed.shape[1])
    returned = lax.all_to_all(summed, "sp", split_axis=0, concat_axis=0, tiled=True)
    returned = returned.reshape(experts * capacity, returned.shape[2])
    picked = lax.dot_general(
        placing, returned, (((0,), (0,)), ((), ())), preferred_element_type=jnp.float32
    )
    picked = picked.reshape(rows, TOPK, picked.shape[1])
    moe = jnp.sum(picked * route_weight[:, :, None], axis=1)
    return (mixed + moe).astype(jnp.bfloat16)


F32 = jnp.float32
BF16 = jnp.bfloat16
GROUPS = 4
VMEM_LIMIT = 67043328


def dot(a, b):
    return jnp.dot(a, b, preferred_element_type=F32)


def layer_kernel(
    nsp, ntp,
    res_hbm, val_hbm, gate_hbm, cw_hbm, cb_hbm, lg_hbm, lb_hbm, ng_hbm, ids_hbm, rw_hbm,
    ow_hbm, eg_hbm, eu_hbm, ed_hbm,
    out_ref,
    res_ref, val_ref, gate_ref, cw_ref, cb_ref, lg_ref, lb_ref, ng_ref, ids_ref, rw_ref,
    ow, wg, wu, wd, pad, wf, conv, mixed, halo_out, halo_in, st_out, st_in, lg_all, lb_all,
    cc, outgoing, arr, hid, part, one, two_out, two, fin, ret, rs_out, rs_in,
    w_sem, halo_s, halo_r, st_s, st_r, ln_s, ln_r, ag_s, ag_r, zs_s, zs_r, rs_s, rs_r,
    x_s, x_r, r_s, r_r, h_s, h_r,
):
    rows, ch = res_ref.shape
    width = ow.shape[0]
    taps = cw_ref.shape[0]
    reach = taps // 2
    edge = halo_in.shape[1]
    cap = outgoing.shape[0] // nsp
    grp = 2 * cap
    last = GROUPS - 1
    me = lax.axis_index("sp")
    t = lax.axis_index("tp")
    z, mi = me // 2, me % 2
    cx, cy = t % 2, t // 2
    tx = cy * 2 + 1 - cx
    ty = (1 - cy) * 2 + cx
    td = (1 - cy) * 2 + 1 - cx
    far_side = z // 2
    inner = (z + far_side) % 2
    sign = 1 - 2 * far_side
    chips = [
        z,
        far_side * last + sign * (1 + inner),
        far_side * last + sign * last,
        far_side * last + sign * (2 - 2 * inner),
    ]
    sib = 2 * z + 1 - mi

    def remote(src, dst, ss, rs, **dev):
        return pltpu.make_async_remote_copy(
            src_ref=src, dst_ref=dst, send_sem=ss, recv_sem=rs,
            device_id=dev, device_id_type=pl.DeviceIdType.MESH,
        )

    smalls = [
        (val_hbm, val_ref), (gate_hbm, gate_ref), (cw_hbm, cw_ref), (cb_hbm, cb_ref),
        (lg_hbm, lg_ref), (lb_hbm, lb_ref), (ids_hbm, ids_ref), (res_hbm, res_ref),
        (ng_hbm, ng_ref), (rw_hbm, rw_ref),
    ]
    staged = [pltpu.make_async_copy(a, b, w_sem.at[4 + n]) for n, (a, b) in enumerate(smalls)]
    for load in staged:
        load.start()
    barrier = pltpu.get_barrier_semaphore()
    for d in range(1, ntp):
        pl.semaphore_signal(barrier, inc=1, device_id={"tp": (t + d) % ntp},
                            device_id_type=pl.DeviceIdType.MESH)
    for d in range(1, nsp):
        pl.semaphore_signal(barrier, inc=1, device_id={"sp": (me + d) % nsp},
                            device_id_type=pl.DeviceIdType.MESH)
    loads = [
        pltpu.make_async_copy(ow_hbm, ow, w_sem.at[0]),
        pltpu.make_async_copy(eg_hbm.at[0], wg, w_sem.at[1]),
        pltpu.make_async_copy(eu_hbm.at[0], wu, w_sem.at[2]),
        pltpu.make_async_copy(ed_hbm.at[0], wd, w_sem.at[3]),
    ]
    for load in loads:
        load.start()

    with jax.named_scope("glu"):
        staged[0].wait()
        staged[1].wait()
        gated = (val_ref[...].astype(F32) * jax.nn.sigmoid(gate_ref[...].astype(F32))).astype(BF16)
        halo_out[0] = gated[rows - edge:]
        halo_out[1] = gated[:edge]
        pad[edge:edge + rows, :] = gated.astype(F32)
        pad[0:edge, :] = jnp.zeros((edge, ch), F32)
        pad[edge + rows:, :] = jnp.zeros((edge, ch), F32)
        for load in staged[2:6]:
            load.wait()
        wf[0:taps, :] = cw_ref[...].astype(F32)
    with jax.named_scope("bar"):
        pl.semaphore_wait(barrier, ntp + nsp - 2)
    to_right = remote(halo_out.at[0], halo_in.at[0], halo_s.at[0], halo_r.at[0], sp=(me + 1) % nsp)
    to_left = remote(halo_out.at[1], halo_in.at[1], halo_s.at[1], halo_r.at[1],
                     sp=(me + nsp - 1) % nsp)

    @pl.when(me < nsp - 1)
    def _():
        to_right.start()

    @pl.when(me > 0)
    def _():
        to_left.start()

    pending = []

    def send(copy):
        copy.start()
        pending.append(copy)

    others = (tx, ty, td)
    for n, to in enumerate(others):
        send(remote(lg_ref, lg_all.at[t], ln_s.at[n], ln_r.at[t], tp=to))
        send(remote(lb_ref, lb_all.at[t], ln_s.at[ntp + n], ln_r.at[ntp + t], tp=to))

    def convolve(low, high):
        for j in range(0, ch, 128):
            total = jnp.zeros((high - low, 128), F32) + cb_ref[:, j:j + 128]
            for tap in range(taps):
                at = low + tap + edge - reach
                total = total + pad[at:at + high - low, j:j + 128] * wf[tap:tap + 1, j:j + 128]
            conv[low:high, j:j + 128] = total

    with jax.named_scope("conv_mid"):
        convolve(edge, rows - edge)

    with jax.named_scope("halo"):
        @pl.when(me > 0)
        def _():
            to_right.wait_recv()
            pad[0:edge, :] = halo_in[0].astype(F32)

        @pl.when(me < nsp - 1)
        def _():
            to_left.wait_recv()
            pad[edge + rows:, :] = halo_in[1].astype(F32)

    with jax.named_scope("conv_edge"):
        convolve(0, edge)
        convolve(rows - edge, rows)

    lane = lax.broadcasted_iota(jnp.int32, (rows, 128), 1)

    def send_totals(which, sums):
        block = jnp.zeros((rows, 128), F32)
        for n, s in enumerate(sums):
            block = jnp.where(lane == n, s, block)
        st_out[which] = block.T[0:8, :]
        for n, to in enumerate(others):
            k = which * ntp
            send(remote(st_out.at[which], st_in.at[which, t], st_s.at[k + n], st_r.at[k + t],
                        tp=to))

    def totals_of(which, b):
        ref = st_in.at[which, b]
        remote(st_out.at[which], ref, st_s.at[0], st_r.at[which * ntp + b], tp=tx).wait_recv()
        return st_in[which, b]

    def upright(block):
        fill = jnp.zeros((128 - block.shape[0], block.shape[1]), F32)
        return jnp.concatenate([block, fill], axis=0).T

    quart = rows // 4

    def quarter(of, q):
        return cc.at[of, pl.ds(q * quart, quart)]

    with jax.named_scope("center"):
        c = conv[...]
        s1 = jnp.sum(c, axis=1, keepdims=True)
        c = c - s1 / ch
        cc[t] = c.astype(BF16)
        for q in (0, 1, 2, 3):
            block = quarter(t, q)
            send(remote(block, block, ag_s.at[q], ag_r.at[2 * q + q % 2], tp=(tx, ty)[q % 2]))
        send_totals(0, (s1, jnp.sum(c * c, axis=1, keepdims=True)))
        for q in (1, 0, 3, 2):
            block = quarter(t, q)
            send(remote(block, block, ag_s.at[4 + q], ag_r.at[2 * q + 1 - q % 2],
                        tp=(ty, tx)[q % 2]))

    def arrived(of, q, n):
        block = quarter(of, q)
        remote(block, block, ag_s.at[0], ag_r.at[n], tp=tx).wait_recv()

    with jax.named_scope("routes"):
        row = lax.broadcasted_iota(jnp.int32, (rows, rows), 0)
        col = lax.broadcasted_iota(jnp.int32, (rows, rows), 1)
        for load in staged[6:]:
            load.wait()
        ids = upright(ids_ref[...].astype(F32)).astype(jnp.int32)
        id0, id1 = ids[:, 0:1], ids[:, 1:2]
        weights = upright(rw_ref[...])
        hit0, hit1 = lane == id0, lane == id1
        named = jnp.where(hit0, 1.0, jnp.where(hit1, 1.0, 0.0)).astype(BF16)
        before = jnp.where(col < row, 1.0, 0.0).astype(BF16)
        rank = dot(before, named)
        rank0 = jnp.sum(jnp.where(hit0, rank, 0.0), axis=1, keepdims=True).astype(jnp.int32)
        rank1 = jnp.sum(jnp.where(hit1, rank, 0.0), axis=1, keepdims=True).astype(jnp.int32)
        slot = lax.broadcasted_iota(jnp.int32, (rows, nsp * cap), 1)
        pick0 = jnp.where(slot == id0 * cap + rank0, 1.0, 0.0)
        pick1 = jnp.where(slot == id1 * cap + rank1, 1.0, 0.0)
        placing = (pick0 + pick1).T.astype(BF16)
        pick0 = pick0.astype(BF16)
        pick1 = pick1.astype(BF16)
        wide = lax.broadcasted_iota(jnp.int32, (rows, nsp * grp), 1)
        lead0, lead1 = id0 * grp + mi * cap + rank0, id1 * grp + mi * cap + rank1
        pick_r = jnp.where(wide == lead0, 1.0, jnp.where(wide == lead1, 1.0, 0.0)).astype(BF16)

    def relay_ag(q):
        of, n, to = ((tx, 2 * q, ty), (ty, 2 * q + 1, tx))[q % 2]
        arrived(of, q, n)
        block = quarter(of, q)
        send(remote(block, block, ag_s.at[8 + q], ag_r.at[8 + q], tp=to))

    def columns(of):
        return ow[pl.ds(pl.multiple_of(of * ch, ch), ch), :]

    with jax.named_scope("relay_a"):
        relay_ag(0)
        relay_ag(1)
    with jax.named_scope("ln_stats"):
        lg_all[t] = lg_ref[...]
        lb_all[t] = lb_ref[...]
        stats = [st_out[0]] + [totals_of(0, b) for b in others]
        total = stats[0] + stats[1] + stats[2] + stats[3]
        mean = total[0:1] / width
        offs = [s[0:1] / ch - mean for s in stats]
        spread = sum(o * o for o in offs)
        rstd = lax.rsqrt((total[1:2] + ch * spread) / width + 1e-05)
        cols = upright(jnp.concatenate([rstd] + [o * rstd for o in offs], axis=0))
        rstd = cols[:, 0:1]

    def project(of, n):
        a = cc[of].astype(F32) * rstd + cols[:, n:n + 1]
        a = jax.nn.silu(a * lg_all[of] + lb_all[of]).astype(BF16)
        return dot(a, columns(of))

    with jax.named_scope("proj_own"):
        loads[0].wait()
        mixed[...] = res_ref[...].astype(F32) + project(t, 1)
    with jax.named_scope("relay_b"):
        relay_ag(2)
        relay_ag(3)
        for n, b in enumerate(others):
            remote(lg_ref, lg_all.at[b], ln_s.at[0], ln_r.at[b], tp=tx).wait_recv()
            remote(lb_ref, lb_all.at[b], ln_s.at[0], ln_r.at[ntp + b], tp=tx).wait_recv()
    with jax.named_scope("proj_x"):
        arrived(tx, 1, 2)
        arrived(tx, 3, 6)
        mixed[...] += project(tx, 2)
    with jax.named_scope("proj_y"):
        arrived(ty, 0, 1)
        arrived(ty, 2, 5)
        mixed[...] += project(ty, 3)
    with jax.named_scope("proj_d"):
        for q in range(4):
            arrived(td, q, 8 + q)
        full = mixed[...] + project(td, 4)
        mixed[...] = full
    with jax.named_scope("pick"):
        sq = jnp.sum(full * full, axis=1, keepdims=True)
        outgoing[...] = dot(placing, (full * ng_ref[...]).astype(BF16)).astype(BF16)

    def piece(n):
        return pl.ds(pl.multiple_of(n * cap, cap), cap)

    def dispatch(e):
        remote(outgoing.at[piece(e)], arr.at[t, piece(me)], zs_s.at[e], zs_r.at[me], sp=e).start()

    def dispatch_chip(c):
        dispatch(2 * c + mi)
        dispatch(2 * c + 1 - mi)

    def dispatch_pair():
        dispatch_chip(far_side * last + sign * 2)
        dispatch_chip(far_side * last + sign * (3 - 3 * inner))

    with jax.named_scope("zsend"):
        dispatch(sib)

        @pl.when(inner == 1)
        def _():
            dispatch_pair()

        arr[t, piece(me), :] = outgoing[piece(me), :]
        send_totals(1, (sq,))

    def rows_of(k):
        return pl.ds(pl.multiple_of(chips[k] * grp, grp), grp)

    def half(k, c):
        return piece(2 * chips[k] + c)

    def pass_on(k, n, of, at, to):
        block = arr.at[of, at]
        send(remote(block, block, x_s.at[6 * k + n], x_r.at[6 * k + n], tp=to))

    def landed(k, n, of, at):
        block = arr.at[of, at]
        remote(block, block, x_s.at[6 * k + n], x_r.at[6 * k + n], tp=tx).wait_recv()

    def came(e):
        remote(outgoing.at[piece(0)], arr.at[t, piece(e)], zs_s.at[0], zs_r.at[e],
               sp=me).wait_recv()

    def share(k):
        if k == 0:
            pass_on(0, 2 * mi, t, piece(me), tx)
            pass_on(0, 2 * mi + 1, t, piece(me), ty)
            came(sib)
            pass_on(0, 2 * (1 - mi), t, piece(sib), tx)
            pass_on(0, 2 * (1 - mi) + 1, t, piece(sib), ty)
            return
        came(2 * chips[k])
        came(2 * chips[k] + 1)
        pass_on(k, 0, t, half(k, 0), tx)
        pass_on(k, 3, t, half(k, 1), ty)
        pass_on(k, 2, t, half(k, 1), tx)
        pass_on(k, 1, t, half(k, 0), ty)

    def relay(k):
        landed(k, 0, tx, half(k, 0))
        pass_on(k, 4, tx, half(k, 0), ty)
        landed(k, 3, ty, half(k, 1))
        pass_on(k, 5, ty, half(k, 1), tx)

    def gather_end(k):
        landed(k, 1, ty, half(k, 0))
        landed(k, 2, tx, half(k, 1))
        landed(k, 4, td, half(k, 0))
        landed(k, 5, td, half(k, 1))

    def scales(k):
        r = lax.rsqrt((st_out[1] + totals_of(1, tx) + totals_of(1, ty) + totals_of(1, td)) / width
                      + 1e-06)[0:1]
        top = r.astype(BF16).astype(F32)
        mid = (r - top).astype(BF16).astype(F32)
        low = r - top - mid
        three = jnp.concatenate([top, mid, low, jnp.zeros((13, rows), F32)], axis=0).astype(BF16)
        picked = dot(three, pick_r)
        picked = picked[0:1] + picked[1:2] + picked[2:3]
        for e in range(nsp):
            rs_out[e] = jnp.broadcast_to(picked[:, e * grp:(e + 1) * grp], (8, grp))
        for d in range(1, nsp):
            e = (me + d) % nsp
            send(remote(rs_out.at[e], rs_in.at[me], rs_s.at[e], rs_r.at[me], sp=e))
        rs_in[me] = rs_out[me]

        @pl.when(inner == 0)
        def _():
            dispatch_pair()

    def dispatch_last(k):
        dispatch_chip(far_side * last + sign * (1 + 2 * inner))

    def row_scale(k):
        for c in range(2):
            e = 2 * chips[k] + c

            def wait(e=e):
                remote(rs_out.at[0], rs_in.at[e], rs_s.at[0], rs_r.at[e], sp=me).wait_recv()

            if k > 0:
                wait()
            else:
                pl.when(c != mi)(wait)
        return upright(rs_in[2 * chips[k]] + rs_in[2 * chips[k] + 1])[:, 0:1]

    depth = wg.shape[1]
    tile = min(256, depth)

    def expert_up(k):
        scale = row_scale(k)

        def up(n, carry):
            at = pl.ds(pl.multiple_of(n * tile, tile), tile)
            g = jnp.zeros((grp, tile), F32)
            u = jnp.zeros((grp, tile), F32)
            for b in range(ntp):
                x = arr[b, rows_of(k), :]
                g = g + dot(x, wg[b * ch:(b + 1) * ch, at])
                u = u + dot(x, wu[b * ch:(b + 1) * ch, at])
            hid[:, at] = (jax.nn.silu(g * scale) * (u * scale)).astype(BF16)
            return carry

        if k == 0:
            loads[1].wait()
            loads[2].wait()
        lax.fori_loop(0, depth // tile, up, 0)

    def expert_down(k):
        def down(b):
            at = pl.ds(pl.multiple_of(b * ch, ch), ch)
            part[b, rows_of(k), :] = dot(hid[...], wd[:, at]).astype(BF16)

        if k == 0:
            loads[3].wait()
        down(td)
        if k > 0:
            first(k, 1, td, 0, tx)
            first(k, 3, td, 1, ty)
        down(tx)
        if k > 0:
            first(k, 0, tx, 0, tx)
        down(ty)
        if k > 0:
            first(k, 2, ty, 1, ty)
        down(t)

    def first(k, n, of, c, to):
        send(remote(part.at[of, half(k, c)], one.at[n % 2, half(k, c)], r_s.at[6 * k + n],
                    r_r.at[6 * k + n], tp=to))

    def reduce_own(k):
        first(k, 1, td, 0, tx)
        first(k, 3, td, 1, ty)
        first(k, 0, tx, 0, tx)
        first(k, 2, ty, 1, ty)

    def summed(m, block):
        remote(block, block, r_s.at[m], r_r.at[m], tp=tx).wait_recv()

    def reduce_mid(k):
        n = 6 * k
        for c, to in ((0, ty), (1, tx)):
            at = half(k, c)
            summed(n + 1 + 2 * c, one.at[1, at])
            two_out[at, :] = (part[to, at, :].astype(F32) + one[1, at, :].astype(F32)).astype(BF16)
            m = n + 4 + c
            send(remote(two_out.at[at], two.at[at], r_s.at[m], r_r.at[m], tp=to))

    def reduce_end(k):
        n = 6 * k
        for c in range(2):
            at = half(k, c)
            summed(n + 2 * c, one.at[0, at])
            summed(n + 4 + c, two.at[at])
            fin[at, :] = (
                part[t, at, :].astype(F32) + one[0, at, :].astype(F32) + two[at, :].astype(F32)
            ).astype(BF16)
            e = 2 * chips[k] + c
            if k > 0:
                send(remote(fin.at[at], ret.at[piece(me)], h_s.at[e], h_r.at[me], sp=e))
        if k == 0:
            send(remote(fin.at[piece(sib)], ret.at[piece(me)], h_s.at[sib], h_r.at[me], sp=sib))
            ret[piece(me), :] = fin[piece(me), :]

    order = [
        (share, 0), (scales, 0), (relay, 0), (share, 1), (dispatch_last, 3), (gather_end, 0),
        (expert_up, 0), (relay, 1), (expert_down, 0), (share, 2), (gather_end, 1), (share, 3),
        (expert_up, 1), (relay, 2), (expert_down, 1), (relay, 3), (gather_end, 2),
        (expert_up, 2), (reduce_mid, 1), (expert_down, 2), (reduce_end, 1), (gather_end, 3),
        (expert_up, 3), (reduce_mid, 2), (expert_down, 3), (reduce_own, 0), (reduce_end, 2),
        (reduce_mid, 3), (reduce_mid, 0), (reduce_end, 3), (reduce_end, 0),
    ]
    for step, k in order:
        with jax.named_scope(step.__name__ + str(k)):
            step(k)

    with jax.named_scope("ret"):
        for d in range(1, nsp):
            e = (me + d) % nsp
            remote(fin.at[piece(0)], ret.at[piece(e)], h_s.at[0], h_r.at[e], sp=me).wait_recv()
    with jax.named_scope("final"):
        back = ret[...]
        moe = dot(pick0, back) * weights[:, 0:1] + dot(pick1, back) * weights[:, 1:2]
        out_ref[...] = (mixed[...] + moe).astype(out_ref.dtype)

    @pl.when(me < nsp - 1)
    def _():
        to_right.wait_send()

    @pl.when(me > 0)
    def _():
        to_left.wait_send()

    for d in range(1, nsp):
        e = (me + d) % nsp
        remote(outgoing.at[piece(e)], arr.at[t, piece(me)], zs_s.at[e], zs_r.at[me],
               sp=e).wait_send()
    for copy in pending:
        copy.wait_send()


def fused(nsp, ntp, *args):
    (residual, glu_value, glu_gate, conv_weight, conv_bias, ln_gain, ln_bias, out_weight,
     norm_gain, route_ids, route_weight, expert_gate, expert_up, expert_down) = args
    rows, ch = residual.shape
    width = out_weight.shape[0]
    depth = expert_gate.shape[2]
    cap = 2 * rows * TOPK // nsp
    slots = nsp * cap
    grp = 2 * cap
    edge = -(-(conv_weight.shape[0] // 2) // 16) * 16
    small = [residual, glu_value, glu_gate, conv_weight]
    small += [a.reshape(1, ch) for a in (conv_bias, ln_gain, ln_bias, norm_gain)]
    small += [route_ids.T, route_weight.T]
    vmem = pl.BlockSpec(memory_space=pltpu.VMEM)
    hbm = pl.BlockSpec(memory_space=pl.ANY)
    dma = lambda n: pltpu.SemaphoreType.DMA((n,))
    return pl.pallas_call(
        functools.partial(layer_kernel, nsp, ntp),
        out_shape=jax.ShapeDtypeStruct((rows, ch), residual.dtype),
        in_specs=[hbm] * 14,
        out_specs=vmem,
        scratch_shapes=[pltpu.VMEM(a.shape, a.dtype) for a in small] + [
            pltpu.VMEM((width, ch), BF16),
            pltpu.VMEM((width, depth), BF16),
            pltpu.VMEM((width, depth), BF16),
            pltpu.VMEM((depth, width), BF16),
            pltpu.VMEM((rows + 2 * edge, ch), F32),
            pltpu.VMEM((-(-conv_weight.shape[0] // 8) * 8, ch), F32),
            pltpu.VMEM((rows, ch), F32),
            pltpu.VMEM((rows, ch), F32),
            pltpu.VMEM((2, edge, ch), BF16),
            pltpu.VMEM((2, edge, ch), BF16),
            pltpu.VMEM((2, 8, rows), F32),
            pltpu.VMEM((2, ntp, 8, rows), F32),
            pltpu.VMEM((ntp, 1, ch), F32),
            pltpu.VMEM((ntp, 1, ch), F32),
            pltpu.VMEM((ntp, rows, ch), BF16),
            pltpu.VMEM((slots, ch), BF16),
            pltpu.VMEM((ntp, slots, ch), BF16),
            pltpu.VMEM((grp, depth), BF16),
            pltpu.VMEM((ntp, slots, ch), BF16),
            pltpu.VMEM((2, slots, ch), BF16),
            pltpu.VMEM((slots, ch), BF16),
            pltpu.VMEM((slots, ch), BF16),
            pltpu.VMEM((slots, ch), BF16),
            pltpu.VMEM((slots, ch), BF16),
            pltpu.VMEM((nsp, 8, grp), F32),
            pltpu.VMEM((nsp, 8, grp), F32),
            dma(14), dma(2), dma(2), dma(2 * ntp), dma(2 * ntp), dma(2 * ntp), dma(2 * ntp),
            dma(12), dma(12), dma(nsp), dma(nsp), dma(nsp), dma(nsp), dma(6 * GROUPS),
            dma(6 * GROUPS), dma(6 * GROUPS), dma(6 * GROUPS), dma(nsp), dma(nsp),
        ],
        compiler_params=pltpu.CompilerParams(
            collective_id=0, has_side_effects=True, vmem_limit_bytes=VMEM_LIMIT
        ),
    )(*small, out_weight, expert_gate, expert_up, expert_down)


def solution(mesh):
    in_specs = (
        P("sp", "tp"),
        P("sp", "tp"),
        P("sp", "tp"),
        P(None, "tp"),
        P("tp"),
        P("tp"),
        P("tp"),
        P(None, "tp"),
        P("tp"),
        P("sp", None),
        P("sp", None),
        P("sp", None, "tp"),
        P("sp", None, "tp"),
        P("sp", "tp", None),
    )
    out_specs = P("sp", "tp")
    nsp, ntp = mesh.shape["sp"], mesh.shape["tp"]
    body = on_device
    if ntp == 4 and nsp == 2 * GROUPS:
        body = functools.partial(fused, nsp, ntp)
    return jax.shard_map(
        body, mesh=mesh, in_specs=in_specs, out_specs=out_specs, check_vma=False
    )
```

```python
import functools

import jax
import jax.numpy as jnp
from jax import lax
from jax.experimental import pallas as pl
from jax.experimental.pallas import tpu as pltpu
from jax.sharding import PartitionSpec as P

TOPK = 2


def with_halo(cells, sides, width):
    for axis, dim in sides:
        count = lax.axis_size(axis)
        ends = count - 1
        head = lax.slice_in_dim(cells, 0, width, axis=dim)
        tail = lax.slice_in_dim(cells, cells.shape[dim] - width, cells.shape[dim], axis=dim)
        cells = jnp.concatenate(
            [
                lax.ppermute(tail, axis, [(i, (i + 1) % count) for i in range(ends)]),
                cells,
                lax.ppermute(head, axis, [((i + 1) % count, i) for i in range(ends)]),
            ],
            axis=dim,
        )
    return cells


def on_device(
    residual,
    glu_value,
    glu_gate,
    conv_weight,
    conv_bias,
    ln_gain,
    ln_bias,
    out_weight,
    norm_gain,
    route_ids,
    route_weight,
    expert_gate,
    expert_up,
    expert_down,
):
    rows = residual.shape[0]
    width_all = out_weight.shape[0]
    gated = (glu_value.astype(jnp.float32) * jax.nn.sigmoid(glu_gate.astype(jnp.float32))).astype(
        jnp.bfloat16
    )
    reach = conv_weight.shape[0] // 2
    padded = with_halo(gated, (("sp", 0),), reach)
    taps = conv_weight.astype(jnp.float32)
    conv = jnp.zeros(gated.shape, jnp.float32) + conv_bias
    for tap in range(conv_weight.shape[0]):
        conv = conv + padded[tap : tap + rows].astype(jnp.float32) * taps[tap]
    totals = lax.psum((jnp.sum(conv, axis=1), jnp.sum(conv * conv, axis=1)), "tp")
    mean = (totals[0] / width_all)[:, None]
    var = (totals[1] / width_all)[:, None] - mean * mean
    act = jax.nn.silu((conv - mean) * lax.rsqrt(var + 1e-05) * ln_gain + ln_bias).astype(
        jnp.bfloat16
    )
    projected = jnp.dot(
        lax.all_gather(act, "tp", axis=1, tiled=True),
        out_weight,
        preferred_element_type=jnp.float32,
    )
    mixed = residual.astype(jnp.float32) + projected
    squares = lax.psum(jnp.sum(mixed * mixed, axis=1), "tp")
    normed = (mixed * lax.rsqrt(squares / width_all + 1e-06)[:, None] * norm_gain).astype(
        jnp.bfloat16
    )
    experts = lax.axis_size("sp")
    capacity = 2 * rows * TOPK // experts
    flat = route_ids.reshape(-1)
    onehot = (flat[:, None] == jnp.arange(experts, dtype=jnp.int32)[None, :]).astype(jnp.int32)
    rank = jnp.sum((jnp.cumsum(onehot, axis=0) - 1) * onehot, axis=1)
    slot_of = flat * capacity + rank
    placing = (slot_of[None, :] == jnp.arange(experts * capacity, dtype=jnp.int32)[:, None]).astype(
        jnp.bfloat16
    )
    copies = jnp.repeat(normed, TOPK, axis=0)
    outgoing = jnp.dot(placing, copies, preferred_element_type=jnp.float32).astype(jnp.bfloat16)
    outgoing = outgoing.reshape(experts, capacity, normed.shape[1])
    arrived = lax.all_to_all(outgoing, "sp", split_axis=0, concat_axis=0, tiled=True)
    arrived = lax.all_gather(
        arrived.reshape(experts * capacity, normed.shape[1]), "tp", axis=1, tiled=True
    )
    gate = jnp.dot(arrived, expert_gate[0], preferred_element_type=jnp.float32)
    up = jnp.dot(arrived, expert_up[0], preferred_element_type=jnp.float32)
    hidden = (jax.nn.silu(gate) * up).astype(jnp.bfloat16)
    partial_out = jnp.dot(hidden, expert_down[0], preferred_element_type=jnp.float32)
    summed = lax.psum_scatter(
        partial_out.astype(jnp.bfloat16), "tp", scatter_dimension=1, tiled=True
    )
    summed = summed.reshape(experts, capacity, summed.shape[1])
    returned = lax.all_to_all(summed, "sp", split_axis=0, concat_axis=0, tiled=True)
    returned = returned.reshape(experts * capacity, returned.shape[2])
    picked = lax.dot_general(
        placing, returned, (((0,), (0,)), ((), ())), preferred_element_type=jnp.float32
    )
    picked = picked.reshape(rows, TOPK, picked.shape[1])
    moe = jnp.sum(picked * route_weight[:, :, None], axis=1)
    return (mixed + moe).astype(jnp.bfloat16)


F32 = jnp.float32
BF16 = jnp.bfloat16
GROUPS = 4
VMEM_LIMIT = 67043328


def dot(a, b):
    return jnp.dot(a, b, preferred_element_type=F32)


def layer_kernel(
    nsp, ntp,
    res_hbm, val_hbm, gate_hbm, cw_hbm, cb_hbm, lg_hbm, lb_hbm, ng_hbm, ids_hbm, rw_hbm,
    ow_hbm, eg_hbm, eu_hbm, ed_hbm,
    out_ref,
    res_ref, val_ref, gate_ref, cw_ref, cb_ref, lg_ref, lb_ref, ng_ref, ids_ref, rw_ref,
    ow, wg, wu, wd, pad, wf, conv, mixed, halo_out, halo_in, st_out, st_in, lg_all, lb_all,
    cc, outgoing, arr, hid, part, one, two_out, two, fin, ret, rs_out, rs_in,
    w_sem, halo_s, halo_r, st_s, st_r, ln_s, ln_r, ag_s, ag_r, zs_s, zs_r, rs_s, rs_r,
    x_s, x_r, r_s, r_r, h_s, h_r,
):
    rows, ch = res_ref.shape
    width = ow.shape[0]
    taps = cw_ref.shape[0]
    reach = taps // 2
    edge = halo_in.shape[1]
    cap = outgoing.shape[0] // nsp
    grp = 2 * cap
    last = GROUPS - 1
    me = lax.axis_index("sp")
    t = lax.axis_index("tp")
    z, mi = me // 2, me % 2
    cx, cy = t % 2, t // 2
    tx = cy * 2 + 1 - cx
    ty = (1 - cy) * 2 + cx
    td = (1 - cy) * 2 + 1 - cx
    far_side = z // 2
    inner = (z + far_side) % 2
    sign = 1 - 2 * far_side
    chips = [
        z,
        far_side * last + sign * (1 + inner),
        far_side * last + sign * last,
        far_side * last + sign * (2 - 2 * inner),
    ]
    sib = 2 * z + 1 - mi

    def remote(src, dst, ss, rs, **dev):
        return pltpu.make_async_remote_copy(
            src_ref=src, dst_ref=dst, send_sem=ss, recv_sem=rs,
            device_id=dev, device_id_type=pl.DeviceIdType.MESH,
        )

    smalls = [
        (val_hbm, val_ref), (gate_hbm, gate_ref), (cw_hbm, cw_ref), (cb_hbm, cb_ref),
        (lg_hbm, lg_ref), (lb_hbm, lb_ref), (ids_hbm, ids_ref), (res_hbm, res_ref),
        (ng_hbm, ng_ref), (rw_hbm, rw_ref),
    ]
    staged = [pltpu.make_async_copy(a, b, w_sem.at[4 + n]) for n, (a, b) in enumerate(smalls)]
    for load in staged:
        load.start()
    barrier = pltpu.get_barrier_semaphore()
    for d in range(1, ntp):
        pl.semaphore_signal(barrier, inc=1, device_id={"tp": (t + d) % ntp},
                            device_id_type=pl.DeviceIdType.MESH)
    for d in range(1, nsp):
        pl.semaphore_signal(barrier, inc=1, device_id={"sp": (me + d) % nsp},
                            device_id_type=pl.DeviceIdType.MESH)
    loads = [
        pltpu.make_async_copy(ow_hbm, ow, w_sem.at[0]),
        pltpu.make_async_copy(eg_hbm.at[0], wg, w_sem.at[1]),
        pltpu.make_async_copy(eu_hbm.at[0], wu, w_sem.at[2]),
        pltpu.make_async_copy(ed_hbm.at[0], wd, w_sem.at[3]),
    ]
    for load in loads:
        load.start()

    with jax.named_scope("glu"):
        staged[0].wait()
        staged[1].wait()
        gated = (val_ref[...].astype(F32) * jax.nn.sigmoid(gate_ref[...].astype(F32))).astype(BF16)
        halo_out[0] = gated[rows - edge:]
        halo_out[1] = gated[:edge]
        pad[edge:edge + rows, :] = gated.astype(F32)
        pad[0:edge, :] = jnp.zeros((edge, ch), F32)
        pad[edge + rows:, :] = jnp.zeros((edge, ch), F32)
        for load in staged[2:6]:
            load.wait()
        wf[0:taps, :] = cw_ref[...].astype(F32)
    with jax.named_scope("bar"):
        pl.semaphore_wait(barrier, ntp + nsp - 2)
    to_right = remote(halo_out.at[0], halo_in.at[0], halo_s.at[0], halo_r.at[0], sp=(me + 1) % nsp)
    to_left = remote(halo_out.at[1], halo_in.at[1], halo_s.at[1], halo_r.at[1],
                     sp=(me + nsp - 1) % nsp)

    @pl.when(me < nsp - 1)
    def _():
        to_right.start()

    @pl.when(me > 0)
    def _():
        to_left.start()

    def send(copy):
        copy.start()

    def drain(ref, sem):
        remote(ref, ref, sem, sem, tp=tx).wait_send()

    def receive(ref, sem):
        remote(ref, ref, sem, sem, tp=tx).wait_recv()

    others = (tx, ty, td)
    for to in others:
        send(remote(lg_ref, lg_all.at[t], ln_s.at[0], ln_r.at[0], tp=to))
        send(remote(lb_ref, lb_all.at[t], ln_s.at[1], ln_r.at[1], tp=to))

    def convolve(low, high):
        for j in range(0, ch, 128):
            total = jnp.zeros((high - low, 128), F32) + cb_ref[:, j:j + 128]
            for tap in range(taps):
                at = low + tap + edge - reach
                total = total + pad[at:at + high - low, j:j + 128] * wf[tap:tap + 1, j:j + 128]
            conv[low:high, j:j + 128] = total

    with jax.named_scope("conv_mid"):
        convolve(edge, rows - edge)

    with jax.named_scope("halo"):
        @pl.when(me > 0)
        def _():
            to_right.wait_recv()
            pad[0:edge, :] = halo_in[0].astype(F32)

        @pl.when(me < nsp - 1)
        def _():
            to_left.wait_recv()
            pad[edge + rows:, :] = halo_in[1].astype(F32)

    with jax.named_scope("conv_edge"):
        convolve(0, edge)
        convolve(rows - edge, rows)

    lane = lax.broadcasted_iota(jnp.int32, (rows, 128), 1)

    def send_totals(which, sums):
        block = jnp.zeros((rows, 128), F32)
        for n, s in enumerate(sums):
            block = jnp.where(lane == n, s, block)
        st_out[which] = block.T[0:8, :]
        for to in others:
            send(remote(st_out.at[which], st_in.at[which, t], st_s.at[0], st_r.at[which], tp=to))

    def totals(which):
        receive(st_in.at[which, pl.ds(0, ntp - 1)], st_r.at[which])
        return [st_out[which]] + [st_in[which, b] for b in others]

    def upright(block):
        fill = jnp.zeros((128 - block.shape[0], block.shape[1]), F32)
        return jnp.concatenate([block, fill], axis=0).T

    quart = rows // 4

    def quarter(of, q):
        return cc.at[of, pl.ds(q * quart, quart)]

    with jax.named_scope("center"):
        c = conv[...]
        s1 = jnp.sum(c, axis=1, keepdims=True)
        c = c - s1 / ch
        cc[t] = c.astype(BF16)
        send_totals(0, (s1, jnp.sum(c * c, axis=1, keepdims=True)))
        for q in (0, 1, 2, 3):
            block = quarter(t, q)
            send(remote(block, block, ag_s.at[0], ag_r.at[q], tp=(tx, ty)[q % 2]))
        for q in (1, 0, 3, 2):
            block = quarter(t, q)
            send(remote(block, block, ag_s.at[0], ag_r.at[5 - q % 2], tp=(ty, tx)[q % 2]))

    with jax.named_scope("routes"):
        row = lax.broadcasted_iota(jnp.int32, (rows, rows), 0)
        col = lax.broadcasted_iota(jnp.int32, (rows, rows), 1)
        for load in staged[6:]:
            load.wait()
        ids = upright(ids_ref[...].astype(F32)).astype(jnp.int32)
        id0, id1 = ids[:, 0:1], ids[:, 1:2]
        weights = upright(rw_ref[...])
        hit0, hit1 = lane == id0, lane == id1
        named = jnp.where(hit0, 1.0, jnp.where(hit1, 1.0, 0.0)).astype(BF16)
        before = jnp.where(col < row, 1.0, 0.0).astype(BF16)
        rank = dot(before, named)
        rank0 = jnp.sum(jnp.where(hit0, rank, 0.0), axis=1, keepdims=True).astype(jnp.int32)
        rank1 = jnp.sum(jnp.where(hit1, rank, 0.0), axis=1, keepdims=True).astype(jnp.int32)
        slot = lax.broadcasted_iota(jnp.int32, (rows, nsp * cap), 1)
        pick0 = jnp.where(slot == id0 * cap + rank0, 1.0, 0.0)
        pick1 = jnp.where(slot == id1 * cap + rank1, 1.0, 0.0)
        placing = (pick0 + pick1).T.astype(BF16)
        pick0 = pick0.astype(BF16)
        pick1 = pick1.astype(BF16)
        wide = lax.broadcasted_iota(jnp.int32, (rows, nsp * grp), 1)
        lead0, lead1 = id0 * grp + mi * cap + rank0, id1 * grp + mi * cap + rank1
        pick_r = jnp.where(wide == lead0, 1.0, jnp.where(wide == lead1, 1.0, 0.0)).astype(BF16)

    def relay_ag(q):
        of, to = ((tx, ty), (ty, tx))[q % 2]
        block = quarter(of, q)
        receive(block, ag_r.at[q])
        send(remote(block, block, ag_s.at[0], ag_r.at[6], tp=to))

    def columns(of):
        return ow[pl.ds(pl.multiple_of(of * ch, ch), ch), :]

    with jax.named_scope("relay_a"):
        relay_ag(0)
        relay_ag(1)
    with jax.named_scope("relay_b"):
        relay_ag(2)
        relay_ag(3)
        receive(lg_all.at[pl.ds(0, ntp - 1)], ln_r.at[0])
        receive(lb_all.at[pl.ds(0, ntp - 1)], ln_r.at[1])
    with jax.named_scope("ln_stats"):
        lg_all[t] = lg_ref[...]
        lb_all[t] = lb_ref[...]
        stats = totals(0)
        total = stats[0] + stats[1] + stats[2] + stats[3]
        mean = total[0:1] / width
        offs = [s[0:1] / ch - mean for s in stats]
        spread = sum(o * o for o in offs)
        rstd = lax.rsqrt((total[1:2] + ch * spread) / width + 1e-05)
        cols = upright(jnp.concatenate([rstd] + [o * rstd for o in offs], axis=0))
        rstd = cols[:, 0:1]

    def project(of, n):
        a = cc[of].astype(F32) * rstd + cols[:, n:n + 1]
        a = jax.nn.silu(a * lg_all[of] + lb_all[of]).astype(BF16)
        return dot(a, columns(of))

    with jax.named_scope("proj_own"):
        loads[0].wait()
        mixed[...] = res_ref[...].astype(F32) + project(t, 1)
    with jax.named_scope("proj_x"):
        receive(cc.at[tx, pl.ds(0, 2 * quart)], ag_r.at[4])
        mixed[...] += project(tx, 2)
    with jax.named_scope("proj_y"):
        receive(cc.at[ty, pl.ds(0, 2 * quart)], ag_r.at[5])
        mixed[...] += project(ty, 3)
    with jax.named_scope("proj_d"):
        receive(cc.at[td], ag_r.at[6])
        full = mixed[...] + project(td, 4)
        mixed[...] = full
    with jax.named_scope("pick"):
        sq = jnp.sum(full * full, axis=1, keepdims=True)
        outgoing[...] = dot(placing, (full * ng_ref[...]).astype(BF16)).astype(BF16)

    def piece(n):
        return pl.ds(pl.multiple_of(n * cap, cap), cap)

    def dispatch(e):
        remote(outgoing.at[piece(e)], arr.at[t, piece(me)], zs_s.at[0], zs_r.at[me], sp=e).start()

    def dispatch_chip(c):
        dispatch(2 * c + mi)
        dispatch(2 * c + 1 - mi)

    def dispatch_pair():
        dispatch_chip(far_side * last + sign * 2)
        dispatch_chip(far_side * last + sign * (3 - 3 * inner))

    with jax.named_scope("zsend"):
        dispatch(sib)

        @pl.when(inner == 1)
        def _():
            dispatch_pair()

        arr[t, piece(me), :] = outgoing[piece(me), :]
        send_totals(1, (sq,))

    def rows_of(k):
        return pl.ds(pl.multiple_of(chips[k] * grp, grp), grp)

    def half(k, c):
        return piece(2 * chips[k] + c)

    def pass_on(k, n, of, at, to):
        block = arr.at[of, at]
        send(remote(block, block, x_s.at[0], x_r.at[3 * k + n], tp=to))

    def share(k):
        for c in (mi, 1 - mi) if k == 0 else (1, 0):
            e = 2 * chips[k] + c
            if k > 0:
                receive(arr.at[t, piece(e)], zs_r.at[e])
            elif c is not mi:
                receive(arr.at[t, piece(e)], zs_r.at[e])
            pass_on(k, 2 * c, t, piece(e), tx)
            pass_on(k, 2 - c, t, piece(e), ty)

    def relay(k):
        receive(arr.at[tx, half(k, 0)], x_r.at[3 * k])
        pass_on(k, 2, tx, half(k, 0), ty)
        receive(arr.at[ty, half(k, 1)], x_r.at[3 * k + 1])
        pass_on(k, 2, ty, half(k, 1), tx)

    def gather_end(k):
        receive(arr.at[0, pl.ds(0, 4 * cap)], x_r.at[3 * k + 2])

    def scales(k):
        r = lax.rsqrt(sum(totals(1)) / width + 1e-06)[0:1]
        top = r.astype(BF16).astype(F32)
        mid = (r - top).astype(BF16).astype(F32)
        low = r - top - mid
        three = jnp.concatenate([top, mid, low, jnp.zeros((13, rows), F32)], axis=0).astype(BF16)
        picked = dot(three, pick_r)
        picked = picked[0:1] + picked[1:2] + picked[2:3]
        for e in range(nsp):
            rs_out[e] = jnp.broadcast_to(picked[:, e * grp:(e + 1) * grp], (8, grp))
        for d in range(1, nsp):
            e = (me + d) % nsp
            send(remote(rs_out.at[e], rs_in.at[me], rs_s.at[0], rs_r.at[z], sp=e))
        rs_in[me] = rs_out[me]

        @pl.when(inner == 0)
        def _():
            dispatch_pair()

    def dispatch_last(k):
        dispatch_chip(far_side * last + sign * (1 + 2 * inner))

    def row_scale(k):
        receive(rs_in.at[pl.ds(0, 2 if k else 1)], rs_r.at[chips[k]])
        return upright(rs_in[2 * chips[k]] + rs_in[2 * chips[k] + 1])[:, 0:1]

    depth = wg.shape[1]
    tile = min(256, depth)

    def expert_up(k):
        scale = row_scale(k)

        def up(n, carry):
            at = pl.ds(pl.multiple_of(n * tile, tile), tile)
            g = jnp.zeros((grp, tile), F32)
            u = jnp.zeros((grp, tile), F32)
            for b in range(ntp):
                x = arr[b, rows_of(k), :]
                g = g + dot(x, wg[b * ch:(b + 1) * ch, at])
                u = u + dot(x, wu[b * ch:(b + 1) * ch, at])
            hid[:, at] = (jax.nn.silu(g * scale) * (u * scale)).astype(BF16)
            return carry

        if k == 0:
            loads[1].wait()
            loads[2].wait()
        lax.fori_loop(0, depth // tile, up, 0)

    def expert_down(k):
        def down(b):
            at = pl.ds(pl.multiple_of(b * ch, ch), ch)
            part[b, rows_of(k), :] = dot(hid[...], wd[:, at]).astype(BF16)

        if k == 0:
            loads[3].wait()
        down(td)
        if k > 0:
            first(k, 1, td, 0, tx)
            first(k, 3, td, 1, ty)
        down(tx)
        if k > 0:
            first(k, 0, tx, 0, tx)
        down(ty)
        if k > 0:
            first(k, 2, ty, 1, ty)
        down(t)

    def first(k, n, of, c, to):
        send(remote(part.at[of, half(k, c)], one.at[n % 2, half(k, c)], r_s.at[0],
                    r_r.at[4 * k + 2 * (1 - n % 2) + c], tp=to))

    def own_far(k):
        first(k, 1, td, 0, tx)
        first(k, 3, td, 1, ty)

    def own_near(k):
        first(k, 0, tx, 0, tx)
        first(k, 2, ty, 1, ty)

    def reduce_mid(k):
        for c, to in ((0, ty), (1, tx)):
            at = half(k, c)
            receive(one.at[1, at], r_r.at[4 * k + c])
            two_out[at, :] = (part[to, at, :].astype(F32) + one[1, at, :].astype(F32)).astype(BF16)
            send(remote(two_out.at[at], two.at[at], r_s.at[0], r_r.at[4 * k + 2 + c], tp=to))

    def reduce_end(k):
        for c in range(2):
            at = half(k, c)
            receive(one.at[0, rows_of(k)], r_r.at[4 * k + 2 + c])
            fin[at, :] = (
                part[t, at, :].astype(F32) + one[0, at, :].astype(F32) + two[at, :].astype(F32)
            ).astype(BF16)
            e = 2 * chips[k] + c
            if k > 0:
                send(remote(fin.at[at], ret.at[piece(me)], h_s.at[0], h_r.at[0], sp=e))
        if k == 0:
            send(remote(fin.at[piece(sib)], ret.at[piece(me)], h_s.at[0], h_r.at[0], sp=sib))
            ret[piece(me), :] = fin[piece(me), :]

    order = [
        (share, 0), (relay, 0), (scales, 0), (share, 1), (dispatch_last, 3), (gather_end, 0),
        (expert_up, 0), (relay, 1), (expert_down, 0), (share, 2), (gather_end, 1), (share, 3),
        (expert_up, 1), (relay, 2), (expert_down, 1), (relay, 3), (gather_end, 2),
        (expert_up, 2), (reduce_mid, 1), (expert_down, 2), (gather_end, 3), (expert_up, 3),
        (reduce_end, 1), (reduce_mid, 2), (expert_down, 3), (own_far, 0), (reduce_end, 2),
        (reduce_mid, 3), (own_near, 0), (reduce_mid, 0), (reduce_end, 3), (reduce_end, 0),
    ]
    for step, k in order:
        with jax.named_scope(step.__name__ + str(k)):
            step(k)

    with jax.named_scope("drain"):
        @pl.when(me < nsp - 1)
        def _():
            to_right.wait_send()

        @pl.when(me > 0)
        def _():
            to_left.wait_send()

        drain(lg_all.at[pl.ds(0, ntp - 1)], ln_s.at[0])
        drain(lb_all.at[pl.ds(0, ntp - 1)], ln_s.at[1])
        drain(rs_out.at[pl.ds(0, 2 * (ntp - 1))], st_s.at[0])
        drain(cc.at[pl.ds(0, 3)], ag_s.at[0])
        drain(outgoing.at[pl.ds(0, (nsp - 1) * cap)], zs_s.at[0])
        drain(rs_out.at[pl.ds(0, nsp - 1)], rs_s.at[0])
        drain(arr.at[pl.ds(0, 3)], x_s.at[0])
        drain(arr.at[pl.ds(0, 3)], r_s.at[0])
    with jax.named_scope("ret"):
        receive(ret.at[pl.ds(0, (nsp - 1) * cap)], h_r.at[0])
    with jax.named_scope("final"):
        back = ret[...]
        moe = dot(pick0, back) * weights[:, 0:1] + dot(pick1, back) * weights[:, 1:2]
        out_ref[...] = (mixed[...] + moe).astype(out_ref.dtype)
        drain(ret.at[pl.ds(0, (nsp - 1) * cap)], h_s.at[0])


def fused(nsp, ntp, *args):
    (residual, glu_value, glu_gate, conv_weight, conv_bias, ln_gain, ln_bias, out_weight,
     norm_gain, route_ids, route_weight, expert_gate, expert_up, expert_down) = args
    rows, ch = residual.shape
    width = out_weight.shape[0]
    depth = expert_gate.shape[2]
    cap = 2 * rows * TOPK // nsp
    slots = nsp * cap
    grp = 2 * cap
    edge = -(-(conv_weight.shape[0] // 2) // 16) * 16
    small = [residual, glu_value, glu_gate, conv_weight]
    small += [a.reshape(1, ch) for a in (conv_bias, ln_gain, ln_bias, norm_gain)]
    small += [route_ids.T, route_weight.T]
    vmem = pl.BlockSpec(memory_space=pltpu.VMEM)
    hbm = pl.BlockSpec(memory_space=pl.ANY)
    dma = lambda n: pltpu.SemaphoreType.DMA((n,))
    return pl.pallas_call(
        functools.partial(layer_kernel, nsp, ntp),
        out_shape=jax.ShapeDtypeStruct((rows, ch), residual.dtype),
        in_specs=[hbm] * 14,
        out_specs=vmem,
        scratch_shapes=[pltpu.VMEM(a.shape, a.dtype) for a in small] + [
            pltpu.VMEM((width, ch), BF16),
            pltpu.VMEM((width, depth), BF16),
            pltpu.VMEM((width, depth), BF16),
            pltpu.VMEM((depth, width), BF16),
            pltpu.VMEM((rows + 2 * edge, ch), F32),
            pltpu.VMEM((-(-conv_weight.shape[0] // 8) * 8, ch), F32),
            pltpu.VMEM((rows, ch), F32),
            pltpu.VMEM((rows, ch), F32),
            pltpu.VMEM((2, edge, ch), BF16),
            pltpu.VMEM((2, edge, ch), BF16),
            pltpu.VMEM((2, 8, rows), F32),
            pltpu.VMEM((2, ntp, 8, rows), F32),
            pltpu.VMEM((ntp, 1, ch), F32),
            pltpu.VMEM((ntp, 1, ch), F32),
            pltpu.VMEM((ntp, rows, ch), BF16),
            pltpu.VMEM((slots, ch), BF16),
            pltpu.VMEM((ntp, slots, ch), BF16),
            pltpu.VMEM((grp, depth), BF16),
            pltpu.VMEM((ntp, slots, ch), BF16),
            pltpu.VMEM((2, slots, ch), BF16),
            pltpu.VMEM((slots, ch), BF16),
            pltpu.VMEM((slots, ch), BF16),
            pltpu.VMEM((slots, ch), BF16),
            pltpu.VMEM((slots, ch), BF16),
            pltpu.VMEM((nsp, 8, grp), F32),
            pltpu.VMEM((nsp, 8, grp), F32),
            dma(14), dma(2), dma(2), dma(1), dma(2), dma(2), dma(2), dma(1), dma(7),
            dma(1), dma(nsp), dma(1), dma(GROUPS), dma(1), dma(3 * GROUPS), dma(1),
            dma(4 * GROUPS), dma(1), dma(1),
        ],
        compiler_params=pltpu.CompilerParams(
            collective_id=0, has_side_effects=True, vmem_limit_bytes=VMEM_LIMIT
        ),
    )(*small, out_weight, expert_gate, expert_up, expert_down)


def solution(mesh):
    in_specs = (
        P("sp", "tp"),
        P("sp", "tp"),
        P("sp", "tp"),
        P(None, "tp"),
        P("tp"),
        P("tp"),
        P("tp"),
        P(None, "tp"),
        P("tp"),
        P("sp", None),
        P("sp", None),
        P("sp", None, "tp"),
        P("sp", None, "tp"),
        P("sp", "tp", None),
    )
    out_specs = P("sp", "tp")
    nsp, ntp = mesh.shape["sp"], mesh.shape["tp"]
    body = on_device
    if ntp == 4 and nsp == 2 * GROUPS:
        body = functools.partial(fused, nsp, ntp)
    return jax.shard_map(
        body, mesh=mesh, in_specs=in_specs, out_specs=out_specs, check_vma=False
    )
```

```python
import functools

import jax
import jax.numpy as jnp
from jax import lax
from jax.experimental import pallas as pl
from jax.experimental.pallas import tpu as pltpu
from jax.sharding import PartitionSpec as P

TOPK = 2


def with_halo(cells, sides, width):
    for axis, dim in sides:
        count = lax.axis_size(axis)
        ends = count - 1
        head = lax.slice_in_dim(cells, 0, width, axis=dim)
        tail = lax.slice_in_dim(cells, cells.shape[dim] - width, cells.shape[dim], axis=dim)
        cells = jnp.concatenate(
            [
                lax.ppermute(tail, axis, [(i, (i + 1) % count) for i in range(ends)]),
                cells,
                lax.ppermute(head, axis, [((i + 1) % count, i) for i in range(ends)]),
            ],
            axis=dim,
        )
    return cells


def on_device(
    residual,
    glu_value,
    glu_gate,
    conv_weight,
    conv_bias,
    ln_gain,
    ln_bias,
    out_weight,
    norm_gain,
    route_ids,
    route_weight,
    expert_gate,
    expert_up,
    expert_down,
):
    rows = residual.shape[0]
    width_all = out_weight.shape[0]
    gated = (glu_value.astype(jnp.float32) * jax.nn.sigmoid(glu_gate.astype(jnp.float32))).astype(
        jnp.bfloat16
    )
    reach = conv_weight.shape[0] // 2
    padded = with_halo(gated, (("sp", 0),), reach)
    taps = conv_weight.astype(jnp.float32)
    conv = jnp.zeros(gated.shape, jnp.float32) + conv_bias
    for tap in range(conv_weight.shape[0]):
        conv = conv + padded[tap : tap + rows].astype(jnp.float32) * taps[tap]
    totals = lax.psum((jnp.sum(conv, axis=1), jnp.sum(conv * conv, axis=1)), "tp")
    mean = (totals[0] / width_all)[:, None]
    var = (totals[1] / width_all)[:, None] - mean * mean
    act = jax.nn.silu((conv - mean) * lax.rsqrt(var + 1e-05) * ln_gain + ln_bias).astype(
        jnp.bfloat16
    )
    projected = jnp.dot(
        lax.all_gather(act, "tp", axis=1, tiled=True),
        out_weight,
        preferred_element_type=jnp.float32,
    )
    mixed = residual.astype(jnp.float32) + projected
    squares = lax.psum(jnp.sum(mixed * mixed, axis=1), "tp")
    normed = (mixed * lax.rsqrt(squares / width_all + 1e-06)[:, None] * norm_gain).astype(
        jnp.bfloat16
    )
    experts = lax.axis_size("sp")
    capacity = 2 * rows * TOPK // experts
    flat = route_ids.reshape(-1)
    onehot = (flat[:, None] == jnp.arange(experts, dtype=jnp.int32)[None, :]).astype(jnp.int32)
    rank = jnp.sum((jnp.cumsum(onehot, axis=0) - 1) * onehot, axis=1)
    slot_of = flat * capacity + rank
    placing = (slot_of[None, :] == jnp.arange(experts * capacity, dtype=jnp.int32)[:, None]).astype(
        jnp.bfloat16
    )
    copies = jnp.repeat(normed, TOPK, axis=0)
    outgoing = jnp.dot(placing, copies, preferred_element_type=jnp.float32).astype(jnp.bfloat16)
    outgoing = outgoing.reshape(experts, capacity, normed.shape[1])
    arrived = lax.all_to_all(outgoing, "sp", split_axis=0, concat_axis=0, tiled=True)
    arrived = lax.all_gather(
        arrived.reshape(experts * capacity, normed.shape[1]), "tp", axis=1, tiled=True
    )
    gate = jnp.dot(arrived, expert_gate[0], preferred_element_type=jnp.float32)
    up = jnp.dot(arrived, expert_up[0], preferred_element_type=jnp.float32)
    hidden = (jax.nn.silu(gate) * up).astype(jnp.bfloat16)
    partial_out = jnp.dot(hidden, expert_down[0], preferred_element_type=jnp.float32)
    summed = lax.psum_scatter(
        partial_out.astype(jnp.bfloat16), "tp", scatter_dimension=1, tiled=True
    )
    summed = summed.reshape(experts, capacity, summed.shape[1])
    returned = lax.all_to_all(summed, "sp", split_axis=0, concat_axis=0, tiled=True)
    returned = returned.reshape(experts * capacity, returned.shape[2])
    picked = lax.dot_general(
        placing, returned, (((0,), (0,)), ((), ())), preferred_element_type=jnp.float32
    )
    picked = picked.reshape(rows, TOPK, picked.shape[1])
    moe = jnp.sum(picked * route_weight[:, :, None], axis=1)
    return (mixed + moe).astype(jnp.bfloat16)


F32 = jnp.float32
BF16 = jnp.bfloat16
GROUPS = 4
VMEM_LIMIT = 67043328


def dot(a, b):
    return jnp.dot(a, b, preferred_element_type=F32)


def layer_kernel(
    nsp, ntp,
    res_hbm, val_hbm, gate_hbm, cw_hbm, cb_hbm, lg_hbm, lb_hbm, ng_hbm, ids_hbm, rw_hbm,
    ow_hbm, eg_hbm, eu_hbm, ed_hbm,
    out_ref,
    res_ref, val_ref, gate_ref, cw_ref, cb_ref, lg_ref, lb_ref, ng_ref, ids_ref, rw_ref,
    ow, wg, wu, wd, pad, wf, conv, mixed, halo_out, halo_in, st_out, st_in, lg_all, lb_all,
    cc, outgoing, arr, hid, part, one, two_out, two, fin, ret, rs_out, rs_in,
    tok, placed, near, whole,
    w_sem, halo_s, halo_r, st_s, st_r, ln_s, ln_r, ag_s, ag_r, zs_s, zs_r, rs_s, rs_r,
    x_s, x_r, r_s, r_r, h_s, h_r,
):
    rows, ch = res_ref.shape
    width = ow.shape[0]
    taps = cw_ref.shape[0]
    reach = taps // 2
    edge = halo_in.shape[1]
    cap = outgoing.shape[0] // nsp
    grp = 2 * cap
    last = GROUPS - 1
    me = lax.axis_index("sp")
    t = lax.axis_index("tp")
    z, mi = me // 2, me % 2
    cx, cy = t % 2, t // 2
    tx = cy * 2 + 1 - cx
    ty = (1 - cy) * 2 + cx
    td = (1 - cy) * 2 + 1 - cx
    far_side = z // 2
    inner = (z + far_side) % 2
    sign = 1 - 2 * far_side
    chips = [
        z,
        far_side * last + sign * last,
        far_side * last + sign * (1 + inner),
        far_side * last + sign * (2 - 2 * inner),
    ]
    sib = 2 * z + 1 - mi

    def remote(src, dst, ss, rs, **dev):
        return pltpu.make_async_remote_copy(
            src_ref=src, dst_ref=dst, send_sem=ss, recv_sem=rs,
            device_id=dev, device_id_type=pl.DeviceIdType.MESH,
        )

    smalls = [
        (val_hbm, val_ref), (gate_hbm, gate_ref), (cw_hbm, cw_ref), (cb_hbm, cb_ref),
        (lg_hbm, lg_ref), (lb_hbm, lb_ref), (ids_hbm, ids_ref), (res_hbm, res_ref),
        (ng_hbm, ng_ref), (rw_hbm, rw_ref),
    ]
    staged = [pltpu.make_async_copy(a, b, w_sem.at[4 + n]) for n, (a, b) in enumerate(smalls)]
    for load in staged:
        load.start()
    barrier = pltpu.get_barrier_semaphore()
    for d in range(1, ntp):
        pl.semaphore_signal(barrier, inc=1, device_id={"tp": (t + d) % ntp},
                            device_id_type=pl.DeviceIdType.MESH)
    for d in range(1, nsp):
        pl.semaphore_signal(barrier, inc=1, device_id={"sp": (me + d) % nsp},
                            device_id_type=pl.DeviceIdType.MESH)
    loads = [
        pltpu.make_async_copy(ow_hbm, ow, w_sem.at[0]),
        pltpu.make_async_copy(eg_hbm.at[0], wg, w_sem.at[1]),
        pltpu.make_async_copy(eu_hbm.at[0], wu, w_sem.at[2]),
        pltpu.make_async_copy(ed_hbm.at[0], wd, w_sem.at[3]),
    ]
    for load in loads:
        load.start()

    with jax.named_scope("glu"):
        staged[0].wait()
        staged[1].wait()
        gated = (val_ref[...].astype(F32) * jax.nn.sigmoid(gate_ref[...].astype(F32))).astype(BF16)
        halo_out[0] = gated[rows - edge:]
        halo_out[1] = gated[:edge]
        pad[edge:edge + rows, :] = gated.astype(F32)
        pad[0:edge, :] = jnp.zeros((edge, ch), F32)
        pad[edge + rows:, :] = jnp.zeros((edge, ch), F32)
        for load in staged[2:6]:
            load.wait()
        wf[0:taps, :] = cw_ref[...].astype(F32)
    with jax.named_scope("bar"):
        pl.semaphore_wait(barrier, ntp + nsp - 2)
    to_right = remote(halo_out.at[0], halo_in.at[0], halo_s.at[0], halo_r.at[0], sp=(me + 1) % nsp)
    to_left = remote(halo_out.at[1], halo_in.at[1], halo_s.at[1], halo_r.at[1],
                     sp=(me + nsp - 1) % nsp)

    @pl.when(me < nsp - 1)
    def _():
        to_right.start()

    @pl.when(me > 0)
    def _():
        to_left.start()

    def send(copy):
        copy.start()

    def drain(ref, sem):
        remote(ref, ref, sem, sem, tp=tx).wait_send()

    def receive(ref, sem):
        remote(ref, ref, sem, sem, tp=tx).wait_recv()

    others = (tx, ty, td)
    for to in others:
        send(remote(lg_ref, lg_all.at[t], ln_s.at[0], ln_r.at[0], tp=to))
        send(remote(lb_ref, lb_all.at[t], ln_s.at[1], ln_r.at[1], tp=to))

    def convolve(low, high):
        for j in range(0, ch, 128):
            total = jnp.zeros((high - low, 128), F32) + cb_ref[:, j:j + 128]
            for tap in range(taps):
                at = low + tap + edge - reach
                total = total + pad[at:at + high - low, j:j + 128] * wf[tap:tap + 1, j:j + 128]
            conv[low:high, j:j + 128] = total

    with jax.named_scope("conv_mid"):
        convolve(edge, rows - edge)

    with jax.named_scope("halo"):
        @pl.when(me > 0)
        def _():
            to_right.wait_recv()
            pad[0:edge, :] = halo_in[0].astype(F32)

        @pl.when(me < nsp - 1)
        def _():
            to_left.wait_recv()
            pad[edge + rows:, :] = halo_in[1].astype(F32)

    with jax.named_scope("conv_edge"):
        convolve(0, edge)
        convolve(rows - edge, rows)

    lane = lax.broadcasted_iota(jnp.int32, (rows, 128), 1)

    def send_totals(which, sums):
        block = jnp.zeros((rows, 128), F32)
        for n, s in enumerate(sums):
            block = jnp.where(lane == n, s, block)
        st_out[which] = block.T[0:8, :]
        for to in others:
            send(remote(st_out.at[which], st_in.at[which, t], st_s.at[0], st_r.at[which], tp=to))

    def totals(which):
        receive(st_in.at[which, pl.ds(0, ntp - 1)], st_r.at[which])
        return [st_out[which]] + [st_in[which, b] for b in others]

    def upright(block):
        fill = jnp.zeros((128 - block.shape[0], block.shape[1]), F32)
        return jnp.concatenate([block, fill], axis=0).T

    quart = rows // 4

    def quarter(of, q):
        return cc.at[of, pl.ds(q * quart, quart)]

    with jax.named_scope("center"):
        c = conv[...]
        s1 = jnp.sum(c, axis=1, keepdims=True)
        c = c - s1 / ch
        cc[t] = c.astype(BF16)
        send_totals(0, (s1, jnp.sum(c * c, axis=1, keepdims=True)))
        for q in (0, 1, 2, 3):
            block = quarter(t, q)
            send(remote(block, block, ag_s.at[0], ag_r.at[q], tp=(tx, ty)[q % 2]))
        for q in (1, 0, 3, 2):
            block = quarter(t, q)
            send(remote(block, block, ag_s.at[0], ag_r.at[5 - q % 2], tp=(ty, tx)[q % 2]))

    with jax.named_scope("routes"):
        row = lax.broadcasted_iota(jnp.int32, (rows, rows), 0)
        col = lax.broadcasted_iota(jnp.int32, (rows, rows), 1)
        for load in staged[6:]:
            load.wait()
        ids = upright(ids_ref[...].astype(F32)).astype(jnp.int32)
        id0, id1 = ids[:, 0:1], ids[:, 1:2]
        weights = upright(rw_ref[...])
        hit0, hit1 = lane == id0, lane == id1
        named = jnp.where(hit0, 1.0, jnp.where(hit1, 1.0, 0.0)).astype(BF16)
        before = jnp.where(col < row, 1.0, 0.0).astype(BF16)
        rank = dot(before, named)
        rank0 = jnp.sum(jnp.where(hit0, rank, 0.0), axis=1, keepdims=True).astype(jnp.int32)
        rank1 = jnp.sum(jnp.where(hit1, rank, 0.0), axis=1, keepdims=True).astype(jnp.int32)
        slot = lax.broadcasted_iota(jnp.int32, (rows, nsp * cap), 1)
        pick0 = jnp.where(slot == id0 * cap + rank0, 1.0, 0.0)
        pick1 = jnp.where(slot == id1 * cap + rank1, 1.0, 0.0)
        placed[...] = (pick0 + pick1).T.astype(BF16)
        pick0 = pick0.astype(BF16)
        pick1 = pick1.astype(BF16)
        wide = lax.broadcasted_iota(jnp.int32, (rows, nsp * grp), 1)
        lead0, lead1 = id0 * grp + mi * cap + rank0, id1 * grp + mi * cap + rank1
        pick_r = jnp.where(wide == lead0, 1.0, jnp.where(wide == lead1, 1.0, 0.0)).astype(BF16)

    def relay_ag(q):
        of, to = ((tx, ty), (ty, tx))[q % 2]
        block = quarter(of, q)
        receive(block, ag_r.at[q])
        send(remote(block, block, ag_s.at[0], ag_r.at[6], tp=to))

    def columns(of):
        return ow[pl.ds(pl.multiple_of(of * ch, ch), ch), :]

    with jax.named_scope("relay_a"):
        relay_ag(0)
        relay_ag(1)
    with jax.named_scope("relay_b"):
        relay_ag(2)
        relay_ag(3)
        receive(lg_all.at[pl.ds(0, ntp - 1)], ln_r.at[0])
        receive(lb_all.at[pl.ds(0, ntp - 1)], ln_r.at[1])
    with jax.named_scope("ln_stats"):
        lg_all[t] = lg_ref[...]
        lb_all[t] = lb_ref[...]
        stats = totals(0)
        total = stats[0] + stats[1] + stats[2] + stats[3]
        mean = total[0:1] / width
        offs = [s[0:1] / ch - mean for s in stats]
        spread = sum(o * o for o in offs)
        rstd = lax.rsqrt((total[1:2] + ch * spread) / width + 1e-05)
        cols = upright(jnp.concatenate([rstd] + [o * rstd for o in offs], axis=0))
        rstd = cols[:, 0:1]

    def project(of, n):
        a = cc[of].astype(F32) * rstd + cols[:, n:n + 1]
        a = jax.nn.silu(a * lg_all[of] + lb_all[of]).astype(BF16)
        return dot(a, columns(of))

    with jax.named_scope("proj_own"):
        loads[0].wait()
        mixed[...] = res_ref[...].astype(F32) + project(t, 1)
    with jax.named_scope("proj_x"):
        receive(cc.at[tx, pl.ds(0, 2 * quart)], ag_r.at[4])
        mixed[...] += project(tx, 2)
    with jax.named_scope("proj_y"):
        receive(cc.at[ty, pl.ds(0, 2 * quart)], ag_r.at[5])
        mixed[...] += project(ty, 3)
    with jax.named_scope("proj_d"):
        receive(cc.at[td], ag_r.at[6])
        full = mixed[...] + project(td, 4)
        mixed[...] = full
    def piece(n):
        return pl.ds(pl.multiple_of(n * cap, cap), cap)

    def pass_on(k, n, block, to):
        send(remote(block, block, x_s.at[0], x_r.at[5 * k + n], tp=to))

    with jax.named_scope("pick"):
        tok[t] = (full * ng_ref[...]).astype(BF16)
        parts = [tok.at[t, pl.ds(q * quart, quart)] for q in range(4)]
        for q in range(4):
            pass_on(0, q, parts[q], (tx, ty)[q % 2])
        for q in range(4):
            pass_on(0, 4, parts[q ^ 1], (tx, ty)[q % 2])
        outgoing[...] = dot(placed[...], tok[t]).astype(BF16)

    def dispatch(e):
        remote(outgoing.at[piece(e)], arr.at[t, piece(me)], zs_s.at[0], zs_r.at[me], sp=e).start()

    def dispatch_chip(c):
        dispatch(2 * c + mi)
        dispatch(2 * c + 1 - mi)

    last_chip = far_side * last + sign * (1 + 2 * inner)
    with jax.named_scope("zsend"):
        dispatch_chip(far_side * last + sign * (3 - 3 * inner))
        dispatch_chip(far_side * last + sign * 2)

        send_totals(1, (jnp.sum(full * full, axis=1, keepdims=True),))

    def rows_of(k):
        return pl.ds(pl.multiple_of(chips[k] * grp, grp), grp)

    def half(k, c):
        return piece(2 * chips[k] + c)

    def way(k, of, q):
        if k == 0:
            return tok.at[of, pl.ds(q * quart, quart)]
        start = 2 * chips[k] * cap + q * (cap // 2)
        return arr.at[of, pl.ds(pl.multiple_of(start, cap // 2), cap // 2)]

    def share(k):
        for c in (1, 0):
            e = 2 * chips[k] + c
            receive(arr.at[t, piece(e)], zs_r.at[e])
            one_way, other = way(k, t, 2 * c), way(k, t, 2 * c + 1)
            pass_on(k, 2 * c, one_way, tx)
            pass_on(k, 2 * c + 1, other, ty)
            pass_on(k, 4, other, tx)
            pass_on(k, 4, one_way, ty)

    def relay(k):
        for q in (2, 3, 0, 1) if k else (0, 1, 2, 3):
            of, to = ((tx, ty), (ty, tx))[q % 2]
            receive(way(k, of, q), x_r.at[5 * k + q])
            pass_on(k, 4, way(k, of, q), to)

    def gather_end(k):
        if k < last:
            receive(arr.at[0, pl.ds(0, 4 * cap)], x_r.at[5 * k + 4])
            return
        for c in (1, 0):
            e = 2 * chips[k] + c
            receive(arr.at[:, piece(e)], zs_r.at[e])

    def place(k):
        to = [me, sib, 2 * last_chip, 2 * last_chip + 1]
        both = jnp.concatenate([placed[piece(e), :] for e in to], axis=0)
        for b in range(ntp):
            rows_b = dot(both, tok[b]).astype(BF16)
            arr[b, piece(me), :] = rows_b[:cap]
            near[b] = rows_b[cap:2 * cap]
            whole[0, b] = rows_b[2 * cap:3 * cap]
            whole[1, b] = rows_b[3 * cap:]
        send(remote(near, arr.at[:, piece(me)], zs_s.at[1], zs_r.at[me], sp=sib))
        for c in (0, 1):
            send(remote(whole.at[c], arr.at[:, piece(me)], zs_s.at[2], zs_r.at[me], sp=to[2 + c]))

    def sibling(k):
        receive(arr.at[:, piece(sib)], zs_r.at[sib])

    def scales(k):
        r = lax.rsqrt(sum(totals(1)) / width + 1e-06)[0:1]
        top = r.astype(BF16).astype(F32)
        mid = (r - top).astype(BF16).astype(F32)
        low = r - top - mid
        three = jnp.concatenate([top, mid, low, jnp.zeros((13, rows), F32)], axis=0).astype(BF16)
        picked = dot(three, pick_r)
        picked = picked[0:1] + picked[1:2] + picked[2:3]
        for e in range(nsp):
            rs_out[e] = jnp.broadcast_to(picked[:, e * grp:(e + 1) * grp], (8, grp))
        for d in range(1, nsp):
            e = (me + d) % nsp
            send(remote(rs_out.at[e], rs_in.at[me], rs_s.at[0], rs_r.at[z], sp=e))
        rs_in[me] = rs_out[me]

    def row_scale(k):
        receive(rs_in.at[pl.ds(0, 2 if k else 1)], rs_r.at[chips[k]])
        return upright(rs_in[2 * chips[k]] + rs_in[2 * chips[k] + 1])[:, 0:1]

    depth = wg.shape[1]
    tile = min(256, depth)

    def expert_up(k):
        scale = row_scale(k)

        def up(n, carry):
            at = pl.ds(pl.multiple_of(n * tile, tile), tile)
            g = jnp.zeros((grp, tile), F32)
            u = jnp.zeros((grp, tile), F32)
            for b in range(ntp):
                x = arr[b, rows_of(k), :]
                g = g + dot(x, wg[b * ch:(b + 1) * ch, at])
                u = u + dot(x, wu[b * ch:(b + 1) * ch, at])
            hid[:, at] = (jax.nn.silu(g * scale) * (u * scale)).astype(BF16)
            return carry

        if k == 0:
            loads[1].wait()
            loads[2].wait()
        lax.fori_loop(0, depth // tile, up, 0)

    def expert_down(k):
        def down(b):
            at = pl.ds(pl.multiple_of(b * ch, ch), ch)
            part[b, rows_of(k), :] = dot(hid[...], wd[:, at]).astype(BF16)

        if k == 0:
            loads[3].wait()
        down(td)
        if k > 0:
            first(k, 1, td, 0, tx)
            first(k, 3, td, 1, ty)
        down(tx)
        if k > 0:
            first(k, 0, tx, 0, tx)
        down(ty)
        if k > 0:
            first(k, 2, ty, 1, ty)
        down(t)

    def sub(k, c, p):
        start = (2 * chips[k] + c) * cap + p * (cap // 2)
        return pl.ds(pl.multiple_of(start, cap // 2), cap // 2)

    def first(k, n, of, c, to):
        if n % 2:
            for p in range(2):
                send(remote(part.at[of, sub(k, c, p)], one.at[1, sub(k, c, p)], r_s.at[0],
                            r_r.at[8 * k + 2 * p + c], tp=to))
        else:
            send(remote(part.at[of, half(k, c)], one.at[0, half(k, c)], r_s.at[0],
                        r_r.at[8 * k + 4 + c], tp=to))

    def own_far(k):
        first(k, 1, td, 0, tx)
        first(k, 3, td, 1, ty)

    def own_near(k):
        first(k, 0, tx, 0, tx)
        first(k, 2, ty, 1, ty)

    def reduce_mid(k):
        for p in range(2):
            for c, to in ((0, ty), (1, tx)):
                at = sub(k, c, p)
                receive(one.at[1, at], r_r.at[8 * k + 2 * p + c])
                two_out[at, :] = (part[to, at, :].astype(F32) + one[1, at, :].astype(F32)).astype(
                    BF16
                )
                send(remote(two_out.at[at], two.at[at], r_s.at[0],
                            r_r.at[8 * k + 4 + 2 * p + c], tp=to))

    def reduce_end(k):
        for p in range(2):
            for c in range(2):
                at = sub(k, c, p)
                if p == 0:
                    receive(one.at[0, pl.ds(0, cap + cap // 2)], r_r.at[8 * k + 4 + c])
                else:
                    receive(two.at[at], r_r.at[8 * k + 6 + c])
                fin[at, :] = (
                    part[t, at, :].astype(F32) + one[0, at, :].astype(F32)
                    + two[at, :].astype(F32)
                ).astype(BF16)
                if k > 0:
                    back = pl.ds(pl.multiple_of(me * cap + p * (cap // 2), cap // 2), cap // 2)
                    send(remote(fin.at[at], ret.at[back], h_s.at[0], h_r.at[0],
                                sp=2 * chips[k] + c))
        if k == 0:
            send(remote(fin.at[piece(sib)], ret.at[piece(me)], h_s.at[0], h_r.at[0], sp=sib))
            ret[piece(me), :] = fin[piece(me), :]

    order = [
        (relay, 0), (share, 1), (gather_end, 0), (scales, 0), (place, 0), (share, 2), (relay, 1),
        (sibling, 0), (expert_up, 0), (expert_down, 0), (gather_end, 1), (relay, 2),
        (expert_up, 1), (expert_down, 1), (gather_end, 2),
        (expert_up, 2), (reduce_mid, 1), (expert_down, 2), (gather_end, 3), (expert_up, 3),
        (reduce_end, 1), (reduce_mid, 2), (expert_down, 3), (own_far, 0), (reduce_end, 2),
        (reduce_mid, 3), (own_near, 0), (reduce_mid, 0), (reduce_end, 3), (reduce_end, 0),
    ]
    for step, k in order:
        with jax.named_scope(step.__name__ + str(k)):
            step(k)

    with jax.named_scope("drain"):
        @pl.when(me < nsp - 1)
        def _():
            to_right.wait_send()

        @pl.when(me > 0)
        def _():
            to_left.wait_send()

        drain(lg_all.at[pl.ds(0, ntp - 1)], ln_s.at[0])
        drain(lb_all.at[pl.ds(0, ntp - 1)], ln_s.at[1])
        drain(rs_out.at[pl.ds(0, 2 * (ntp - 1))], st_s.at[0])
        drain(cc.at[pl.ds(0, 3)], ag_s.at[0])
        drain(outgoing.at[pl.ds(0, 4 * cap)], zs_s.at[0])
        drain(whole, zs_s.at[2])
        drain(near, zs_s.at[1])
        drain(rs_out.at[pl.ds(0, nsp - 1)], rs_s.at[0])
        drain(arr.at[pl.ds(0, 3), pl.ds(0, 6 * cap)], x_s.at[0])
        drain(arr.at[pl.ds(0, 3)], r_s.at[0])
    with jax.named_scope("ret"):
        receive(ret.at[pl.ds(0, (nsp - 1) * cap)], h_r.at[0])
    with jax.named_scope("final"):
        back = ret[...]
        moe = dot(pick0, back) * weights[:, 0:1] + dot(pick1, back) * weights[:, 1:2]
        out_ref[...] = (mixed[...] + moe).astype(out_ref.dtype)
        drain(ret.at[pl.ds(0, (nsp - 1) * cap)], h_s.at[0])


def fused(nsp, ntp, *args):
    (residual, glu_value, glu_gate, conv_weight, conv_bias, ln_gain, ln_bias, out_weight,
     norm_gain, route_ids, route_weight, expert_gate, expert_up, expert_down) = args
    rows, ch = residual.shape
    width = out_weight.shape[0]
    depth = expert_gate.shape[2]
    cap = 2 * rows * TOPK // nsp
    slots = nsp * cap
    grp = 2 * cap
    edge = -(-(conv_weight.shape[0] // 2) // 16) * 16
    small = [residual, glu_value, glu_gate, conv_weight]
    small += [a.reshape(1, ch) for a in (conv_bias, ln_gain, ln_bias, norm_gain)]
    small += [route_ids.T, route_weight.T]
    vmem = pl.BlockSpec(memory_space=pltpu.VMEM)
    hbm = pl.BlockSpec(memory_space=pl.ANY)
    dma = lambda n: pltpu.SemaphoreType.DMA((n,))
    return pl.pallas_call(
        functools.partial(layer_kernel, nsp, ntp),
        out_shape=jax.ShapeDtypeStruct((rows, ch), residual.dtype),
        in_specs=[hbm] * 14,
        out_specs=vmem,
        scratch_shapes=[pltpu.VMEM(a.shape, a.dtype) for a in small] + [
            pltpu.VMEM((width, ch), BF16),
            pltpu.VMEM((width, depth), BF16),
            pltpu.VMEM((width, depth), BF16),
            pltpu.VMEM((depth, width), BF16),
            pltpu.VMEM((rows + 2 * edge, ch), F32),
            pltpu.VMEM((-(-conv_weight.shape[0] // 8) * 8, ch), F32),
            pltpu.VMEM((rows, ch), F32),
            pltpu.VMEM((rows, ch), F32),
            pltpu.VMEM((2, edge, ch), BF16),
            pltpu.VMEM((2, edge, ch), BF16),
            pltpu.VMEM((2, 8, rows), F32),
            pltpu.VMEM((2, ntp, 8, rows), F32),
            pltpu.VMEM((ntp, 1, ch), F32),
            pltpu.VMEM((ntp, 1, ch), F32),
            pltpu.VMEM((ntp, rows, ch), BF16),
            pltpu.VMEM((slots, ch), BF16),
            pltpu.VMEM((ntp, slots, ch), BF16),
            pltpu.VMEM((grp, depth), BF16),
            pltpu.VMEM((ntp, slots, ch), BF16),
            pltpu.VMEM((2, slots, ch), BF16),
            pltpu.VMEM((slots, ch), BF16),
            pltpu.VMEM((slots, ch), BF16),
            pltpu.VMEM((slots, ch), BF16),
            pltpu.VMEM((slots, ch), BF16),
            pltpu.VMEM((nsp, 8, grp), F32),
            pltpu.VMEM((nsp, 8, grp), F32),
            pltpu.VMEM((ntp, rows, ch), BF16),
            pltpu.VMEM((slots, rows), BF16),
            pltpu.VMEM((ntp, cap, ch), BF16),
            pltpu.VMEM((2, ntp, cap, ch), BF16),
            dma(14), dma(2), dma(2), dma(1), dma(2), dma(2), dma(2), dma(1), dma(7),
            dma(3), dma(nsp), dma(1), dma(GROUPS), dma(1), dma(5 * GROUPS - 5), dma(1),
            dma(8 * GROUPS), dma(1), dma(1),
        ],
        compiler_params=pltpu.CompilerParams(
            collective_id=0, has_side_effects=True, vmem_limit_bytes=VMEM_LIMIT
        ),
    )(*small, out_weight, expert_gate, expert_up, expert_down)


def solution(mesh):
    in_specs = (
        P("sp", "tp"),
        P("sp", "tp"),
        P("sp", "tp"),
        P(None, "tp"),
        P("tp"),
        P("tp"),
        P("tp"),
        P(None, "tp"),
        P("tp"),
        P("sp", None),
        P("sp", None),
        P("sp", None, "tp"),
        P("sp", None, "tp"),
        P("sp", "tp", None),
    )
    out_specs = P("sp", "tp")
    nsp, ntp = mesh.shape["sp"], mesh.shape["tp"]
    body = on_device
    if ntp == 4 and nsp == 2 * GROUPS:
        body = functools.partial(fused, nsp, ntp)
    return jax.shard_map(
        body, mesh=mesh, in_specs=in_specs, out_specs=out_specs, check_vma=False
    )
```

```python
import functools

import jax
import jax.numpy as jnp
from jax import lax
from jax.experimental import pallas as pl
from jax.experimental.pallas import tpu as pltpu
from jax.sharding import PartitionSpec as P

TOPK = 2


def with_halo(cells, sides, width):
    for axis, dim in sides:
        count = lax.axis_size(axis)
        ends = count - 1
        head = lax.slice_in_dim(cells, 0, width, axis=dim)
        tail = lax.slice_in_dim(cells, cells.shape[dim] - width, cells.shape[dim], axis=dim)
        cells = jnp.concatenate(
            [
                lax.ppermute(tail, axis, [(i, (i + 1) % count) for i in range(ends)]),
                cells,
                lax.ppermute(head, axis, [((i + 1) % count, i) for i in range(ends)]),
            ],
            axis=dim,
        )
    return cells


def on_device(
    residual,
    glu_value,
    glu_gate,
    conv_weight,
    conv_bias,
    ln_gain,
    ln_bias,
    out_weight,
    norm_gain,
    route_ids,
    route_weight,
    expert_gate,
    expert_up,
    expert_down,
):
    rows = residual.shape[0]
    width_all = out_weight.shape[0]
    gated = (glu_value.astype(jnp.float32) * jax.nn.sigmoid(glu_gate.astype(jnp.float32))).astype(
        jnp.bfloat16
    )
    reach = conv_weight.shape[0] // 2
    padded = with_halo(gated, (("sp", 0),), reach)
    taps = conv_weight.astype(jnp.float32)
    conv = jnp.zeros(gated.shape, jnp.float32) + conv_bias
    for tap in range(conv_weight.shape[0]):
        conv = conv + padded[tap : tap + rows].astype(jnp.float32) * taps[tap]
    totals = lax.psum((jnp.sum(conv, axis=1), jnp.sum(conv * conv, axis=1)), "tp")
    mean = (totals[0] / width_all)[:, None]
    var = (totals[1] / width_all)[:, None] - mean * mean
    act = jax.nn.silu((conv - mean) * lax.rsqrt(var + 1e-05) * ln_gain + ln_bias).astype(
        jnp.bfloat16
    )
    projected = jnp.dot(
        lax.all_gather(act, "tp", axis=1, tiled=True),
        out_weight,
        preferred_element_type=jnp.float32,
    )
    mixed = residual.astype(jnp.float32) + projected
    squares = lax.psum(jnp.sum(mixed * mixed, axis=1), "tp")
    normed = (mixed * lax.rsqrt(squares / width_all + 1e-06)[:, None] * norm_gain).astype(
        jnp.bfloat16
    )
    experts = lax.axis_size("sp")
    capacity = 2 * rows * TOPK // experts
    flat = route_ids.reshape(-1)
    onehot = (flat[:, None] == jnp.arange(experts, dtype=jnp.int32)[None, :]).astype(jnp.int32)
    rank = jnp.sum((jnp.cumsum(onehot, axis=0) - 1) * onehot, axis=1)
    slot_of = flat * capacity + rank
    placing = (slot_of[None, :] == jnp.arange(experts * capacity, dtype=jnp.int32)[:, None]).astype(
        jnp.bfloat16
    )
    copies = jnp.repeat(normed, TOPK, axis=0)
    outgoing = jnp.dot(placing, copies, preferred_element_type=jnp.float32).astype(jnp.bfloat16)
    outgoing = outgoing.reshape(experts, capacity, normed.shape[1])
    arrived = lax.all_to_all(outgoing, "sp", split_axis=0, concat_axis=0, tiled=True)
    arrived = lax.all_gather(
        arrived.reshape(experts * capacity, normed.shape[1]), "tp", axis=1, tiled=True
    )
    gate = jnp.dot(arrived, expert_gate[0], preferred_element_type=jnp.float32)
    up = jnp.dot(arrived, expert_up[0], preferred_element_type=jnp.float32)
    hidden = (jax.nn.silu(gate) * up).astype(jnp.bfloat16)
    partial_out = jnp.dot(hidden, expert_down[0], preferred_element_type=jnp.float32)
    summed = lax.psum_scatter(
        partial_out.astype(jnp.bfloat16), "tp", scatter_dimension=1, tiled=True
    )
    summed = summed.reshape(experts, capacity, summed.shape[1])
    returned = lax.all_to_all(summed, "sp", split_axis=0, concat_axis=0, tiled=True)
    returned = returned.reshape(experts * capacity, returned.shape[2])
    picked = lax.dot_general(
        placing, returned, (((0,), (0,)), ((), ())), preferred_element_type=jnp.float32
    )
    picked = picked.reshape(rows, TOPK, picked.shape[1])
    moe = jnp.sum(picked * route_weight[:, :, None], axis=1)
    return (mixed + moe).astype(jnp.bfloat16)


F32 = jnp.float32
BF16 = jnp.bfloat16
GROUPS = 4
VMEM_LIMIT = 67043328


def dot(a, b):
    return jnp.dot(a, b, preferred_element_type=F32)


def layer_kernel(
    nsp, ntp,
    res_hbm, val_hbm, gate_hbm, cw_hbm, cb_hbm, lg_hbm, lb_hbm, ng_hbm, ids_hbm, rw_hbm,
    ow_hbm, eg_hbm, eu_hbm, ed_hbm,
    out_ref,
    res_ref, val_ref, gate_ref, cw_ref, cb_ref, lg_ref, lb_ref, ng_ref, ids_ref, rw_ref,
    ow, wg, wu, wd, pad, wf, conv, mixed, halo_out, halo_in, st_out, st_in, lg_all, lb_all,
    cc, outgoing, arr, hid, part, one, two_out, two, fin, ret, rs_out, rs_in,
    tok, placed, near, whole,
    here, w_sem, halo_s, halo_r, st_s, st_r, ln_s, ln_r, ag_s, ag_r, zs_s, zs_r, rs_s, rs_r,
    x_s, x_r, r_s, r_r, h_s, h_r,
):
    rows, ch = res_ref.shape
    width = ow.shape[0]
    taps = cw_ref.shape[0]
    reach = taps // 2
    edge = halo_in.shape[1]
    cap = outgoing.shape[0] // nsp
    grp = 2 * cap
    last = GROUPS - 1
    me = lax.axis_index("sp")
    t = lax.axis_index("tp")
    z, mi = me // 2, me % 2
    cx, cy = t % 2, t // 2
    tx = cy * 2 + 1 - cx
    ty = (1 - cy) * 2 + cx
    td = (1 - cy) * 2 + 1 - cx
    far_side = z // 2
    inner = (z + far_side) % 2
    sign = 1 - 2 * far_side
    chips = [
        z,
        far_side * last + sign * last,
        far_side * last + sign * (1 + inner),
        far_side * last + sign * (2 - 2 * inner),
    ]
    sib = 2 * z + 1 - mi

    def remote(src, dst, ss, rs, **dev):
        return pltpu.make_async_remote_copy(
            src_ref=src, dst_ref=dst, send_sem=ss, recv_sem=rs,
            device_id=dev, device_id_type=pl.DeviceIdType.MESH,
        )

    smalls = [
        (val_hbm, val_ref), (gate_hbm, gate_ref), (cw_hbm, cw_ref), (cb_hbm, cb_ref),
        (lg_hbm, lg_ref), (lb_hbm, lb_ref), (ids_hbm, ids_ref), (res_hbm, res_ref),
        (ng_hbm, ng_ref), (rw_hbm, rw_ref),
    ]
    staged = [pltpu.make_async_copy(a, b, w_sem.at[4 + n]) for n, (a, b) in enumerate(smalls)]
    for load in staged:
        load.start()
    barrier = pltpu.get_barrier_semaphore()

    def signal(sem, **dev):
        pl.semaphore_signal(sem, inc=1, device_id=dev, device_id_type=pl.DeviceIdType.MESH)

    def along(d, act):
        pl.when(me >= d)(lambda: act(me - d))
        pl.when(me < nsp - d)(lambda: act(me + d))

    def present(d):
        return (me + nsp - d) // nsp + (2 * nsp - 1 - d - me) // nsp

    signal(barrier, tp=tx)
    signal(barrier, tp=ty)
    along(1, lambda e: signal(barrier, sp=e))
    loads = [
        pltpu.make_async_copy(ow_hbm, ow, w_sem.at[0]),
        pltpu.make_async_copy(eg_hbm.at[0], wg, w_sem.at[1]),
        pltpu.make_async_copy(eu_hbm.at[0], wu, w_sem.at[2]),
        pltpu.make_async_copy(ed_hbm.at[0], wd, w_sem.at[3]),
    ]
    for load in loads:
        load.start()

    with jax.named_scope("glu"):
        staged[0].wait()
        staged[1].wait()
        gated = (val_ref[...].astype(F32) * jax.nn.sigmoid(gate_ref[...].astype(F32))).astype(BF16)
        halo_out[0] = gated[rows - edge:]
        halo_out[1] = gated[:edge]
        pad[edge:edge + rows, :] = gated.astype(F32)
        pad[0:edge, :] = jnp.zeros((edge, ch), F32)
        pad[edge + rows:, :] = jnp.zeros((edge, ch), F32)
        for load in staged[2:6]:
            load.wait()
        wf[0:taps, :] = cw_ref[...].astype(F32)
    with jax.named_scope("bar"):
        pl.semaphore_wait(barrier, 2 + present(1))
    to_right = remote(halo_out.at[0], halo_in.at[0], halo_s.at[0], halo_r.at[0], sp=(me + 1) % nsp)
    to_left = remote(halo_out.at[1], halo_in.at[1], halo_s.at[1], halo_r.at[1],
                     sp=(me + nsp - 1) % nsp)

    @pl.when(me < nsp - 1)
    def _():
        to_right.start()

    @pl.when(me > 0)
    def _():
        to_left.start()

    def send(copy):
        copy.start()

    def drain(ref, sem):
        remote(ref, ref, sem, sem, tp=tx).wait_send()

    def receive(ref, sem):
        remote(ref, ref, sem, sem, tp=tx).wait_recv()

    others = (tx, ty, td)

    def send_ln(to):
        send(remote(lg_ref, lg_all.at[t], ln_s.at[0], ln_r.at[0], tp=to))
        send(remote(lb_ref, lb_all.at[t], ln_s.at[1], ln_r.at[1], tp=to))

    signal(here.at[0], tp=tx)
    along(1, lambda e: signal(here.at[1], sp=e))
    send_ln(tx)
    send_ln(ty)

    def heard(n):
        pl.semaphore_wait(here.at[1 + n // 2], present(n))
        if n < 4:
            along(2 * n, lambda e: signal(here.at[1 + n], sp=e))

    def convolve(low, high):
        for j in range(0, ch, 128):
            total = jnp.zeros((high - low, 128), F32) + cb_ref[:, j:j + 128]
            for tap in range(taps):
                at = low + tap + edge - reach
                total = total + pad[at:at + high - low, j:j + 128] * wf[tap:tap + 1, j:j + 128]
            conv[low:high, j:j + 128] = total

    with jax.named_scope("conv_mid"):
        convolve(edge, rows - edge)

    with jax.named_scope("halo"):
        pl.semaphore_wait(here.at[0], 1)
        send_ln(td)

        @pl.when(me > 0)
        def _():
            to_right.wait_recv()
            pad[0:edge, :] = halo_in[0].astype(F32)

        @pl.when(me < nsp - 1)
        def _():
            to_left.wait_recv()
            pad[edge + rows:, :] = halo_in[1].astype(F32)

        heard(1)

    with jax.named_scope("conv_edge"):
        convolve(0, edge)
        convolve(rows - edge, rows)

    lane = lax.broadcasted_iota(jnp.int32, (rows, 128), 1)

    def send_totals(which, sums):
        block = jnp.zeros((rows, 128), F32)
        for n, s in enumerate(sums):
            block = jnp.where(lane == n, s, block)
        st_out[which] = block.T[0:8, :]
        for to in others:
            send(remote(st_out.at[which], st_in.at[which, t], st_s.at[0], st_r.at[which], tp=to))

    def totals(which):
        receive(st_in.at[which, pl.ds(0, ntp - 1)], st_r.at[which])
        return [st_out[which]] + [st_in[which, b] for b in others]

    def upright(block):
        fill = jnp.zeros((128 - block.shape[0], block.shape[1]), F32)
        return jnp.concatenate([block, fill], axis=0).T

    quart = rows // 4

    def quarter(of, q):
        return cc.at[of, pl.ds(q * quart, quart)]

    with jax.named_scope("center"):
        c = conv[...]
        s1 = jnp.sum(c, axis=1, keepdims=True)
        c = c - s1 / ch
        cc[t] = c.astype(BF16)
        send_totals(0, (s1, jnp.sum(c * c, axis=1, keepdims=True)))
        for q in (0, 1, 2, 3):
            block = quarter(t, q)
            send(remote(block, block, ag_s.at[0], ag_r.at[q], tp=(tx, ty)[q % 2]))
        for q in (1, 0, 3, 2):
            block = quarter(t, q)
            send(remote(block, block, ag_s.at[0], ag_r.at[5 - q % 2], tp=(ty, tx)[q % 2]))

    with jax.named_scope("routes"):
        row = lax.broadcasted_iota(jnp.int32, (rows, rows), 0)
        col = lax.broadcasted_iota(jnp.int32, (rows, rows), 1)
        for load in staged[6:]:
            load.wait()
        ids = upright(ids_ref[...].astype(F32)).astype(jnp.int32)
        id0, id1 = ids[:, 0:1], ids[:, 1:2]
        weights = upright(rw_ref[...])
        hit0, hit1 = lane == id0, lane == id1
        named = jnp.where(hit0, 1.0, jnp.where(hit1, 1.0, 0.0)).astype(BF16)
        before = jnp.where(col < row, 1.0, 0.0).astype(BF16)
        rank = dot(before, named)
        rank0 = jnp.sum(jnp.where(hit0, rank, 0.0), axis=1, keepdims=True).astype(jnp.int32)
        rank1 = jnp.sum(jnp.where(hit1, rank, 0.0), axis=1, keepdims=True).astype(jnp.int32)
        slot = lax.broadcasted_iota(jnp.int32, (rows, nsp * cap), 1)
        pick0 = jnp.where(slot == id0 * cap + rank0, 1.0, 0.0)
        pick1 = jnp.where(slot == id1 * cap + rank1, 1.0, 0.0)
        placed[...] = (pick0 + pick1).T.astype(BF16)
        pick0 = pick0.astype(BF16)
        pick1 = pick1.astype(BF16)
        wide = lax.broadcasted_iota(jnp.int32, (rows, nsp * grp), 1)
        lead0, lead1 = id0 * grp + mi * cap + rank0, id1 * grp + mi * cap + rank1
        pick_r = jnp.where(wide == lead0, 1.0, jnp.where(wide == lead1, 1.0, 0.0)).astype(BF16)

    def relay_ag(q):
        of, to = ((tx, ty), (ty, tx))[q % 2]
        block = quarter(of, q)
        receive(block, ag_r.at[q])
        send(remote(block, block, ag_s.at[0], ag_r.at[6], tp=to))

    def columns(of):
        return ow[pl.ds(pl.multiple_of(of * ch, ch), ch), :]

    with jax.named_scope("relay_a"):
        relay_ag(0)
        relay_ag(1)
        heard(2)
    with jax.named_scope("relay_b"):
        relay_ag(2)
        relay_ag(3)
        receive(lg_all.at[pl.ds(0, ntp - 1)], ln_r.at[0])
        receive(lb_all.at[pl.ds(0, ntp - 1)], ln_r.at[1])
    with jax.named_scope("ln_stats"):
        lg_all[t] = lg_ref[...]
        lb_all[t] = lb_ref[...]
        stats = totals(0)
        total = stats[0] + stats[1] + stats[2] + stats[3]
        mean = total[0:1] / width
        offs = [s[0:1] / ch - mean for s in stats]
        spread = sum(o * o for o in offs)
        rstd = lax.rsqrt((total[1:2] + ch * spread) / width + 1e-05)
        cols = upright(jnp.concatenate([rstd] + [o * rstd for o in offs], axis=0))
        rstd = cols[:, 0:1]

    def project(of, n):
        a = cc[of].astype(F32) * rstd + cols[:, n:n + 1]
        a = jax.nn.silu(a * lg_all[of] + lb_all[of]).astype(BF16)
        return dot(a, columns(of))

    with jax.named_scope("proj_own"):
        loads[0].wait()
        mixed[...] = res_ref[...].astype(F32) + project(t, 1)
    with jax.named_scope("proj_x"):
        receive(cc.at[tx, pl.ds(0, 2 * quart)], ag_r.at[4])
        mixed[...] += project(tx, 2)
    with jax.named_scope("proj_y"):
        receive(cc.at[ty, pl.ds(0, 2 * quart)], ag_r.at[5])
        mixed[...] += project(ty, 3)
        heard(4)
    with jax.named_scope("proj_d"):
        receive(cc.at[td], ag_r.at[6])
        full = mixed[...] + project(td, 4)
        mixed[...] = full
    def piece(n):
        return pl.ds(pl.multiple_of(n * cap, cap), cap)

    def pass_on(k, n, block, to):
        send(remote(block, block, x_s.at[0], x_r.at[5 * k + n], tp=to))

    with jax.named_scope("pick"):
        tok[t] = (full * ng_ref[...]).astype(BF16)
        parts = [tok.at[t, pl.ds(q * quart, quart)] for q in range(4)]
        for q in range(4):
            pass_on(0, q, parts[q], (tx, ty)[q % 2])
        for q in range(4):
            pass_on(0, 4, parts[q ^ 1], (tx, ty)[q % 2])
        outgoing[...] = dot(placed[...], tok[t]).astype(BF16)

    def dispatch(e):
        remote(outgoing.at[piece(e)], arr.at[t, piece(me)], zs_s.at[0], zs_r.at[me], sp=e).start()

    def dispatch_chip(c):
        dispatch(2 * c + mi)
        dispatch(2 * c + 1 - mi)

    last_chip = far_side * last + sign * (1 + 2 * inner)
    with jax.named_scope("zsend"):
        dispatch_chip(far_side * last + sign * (3 - 3 * inner))
        dispatch_chip(far_side * last + sign * 2)

        send_totals(1, (jnp.sum(full * full, axis=1, keepdims=True),))

    def rows_of(k):
        return pl.ds(pl.multiple_of(chips[k] * grp, grp), grp)

    def half(k, c):
        return piece(2 * chips[k] + c)

    def way(k, of, q):
        if k == 0:
            return tok.at[of, pl.ds(q * quart, quart)]
        start = 2 * chips[k] * cap + q * (cap // 2)
        return arr.at[of, pl.ds(pl.multiple_of(start, cap // 2), cap // 2)]

    def share(k):
        for c in (1, 0):
            e = 2 * chips[k] + c
            receive(arr.at[t, piece(e)], zs_r.at[e])
            one_way, other = way(k, t, 2 * c), way(k, t, 2 * c + 1)
            pass_on(k, 2 * c, one_way, tx)
            pass_on(k, 2 * c + 1, other, ty)
            pass_on(k, 4, other, tx)
            pass_on(k, 4, one_way, ty)

    def relay(k):
        for q in (2, 3, 0, 1) if k else (0, 1, 2, 3):
            of, to = ((tx, ty), (ty, tx))[q % 2]
            receive(way(k, of, q), x_r.at[5 * k + q])
            pass_on(k, 4, way(k, of, q), to)

    def gather_end(k):
        if k < last:
            receive(arr.at[0, pl.ds(0, 4 * cap)], x_r.at[5 * k + 4])
            return
        for c in (1, 0):
            e = 2 * chips[k] + c
            receive(arr.at[:, piece(e)], zs_r.at[e])

    def place(k):
        to = [me, sib, 2 * last_chip, 2 * last_chip + 1]
        both = jnp.concatenate([placed[piece(e), :] for e in to], axis=0)
        for b in range(ntp):
            rows_b = dot(both, tok[b]).astype(BF16)
            arr[b, piece(me), :] = rows_b[:cap]
            near[b] = rows_b[cap:2 * cap]
            whole[0, b] = rows_b[2 * cap:3 * cap]
            whole[1, b] = rows_b[3 * cap:]
        send(remote(near, arr.at[:, piece(me)], zs_s.at[1], zs_r.at[me], sp=sib))
        for c in (0, 1):
            send(remote(whole.at[c], arr.at[:, piece(me)], zs_s.at[2], zs_r.at[me], sp=to[2 + c]))

    def sibling(k):
        receive(arr.at[:, piece(sib)], zs_r.at[sib])

    def scales(k):
        r = lax.rsqrt(sum(totals(1)) / width + 1e-06)[0:1]
        top = r.astype(BF16).astype(F32)
        mid = (r - top).astype(BF16).astype(F32)
        low = r - top - mid
        three = jnp.concatenate([top, mid, low, jnp.zeros((13, rows), F32)], axis=0).astype(BF16)
        picked = dot(three, pick_r)
        picked = picked[0:1] + picked[1:2] + picked[2:3]
        for e in range(nsp):
            rs_out[e] = jnp.broadcast_to(picked[:, e * grp:(e + 1) * grp], (8, grp))
        for d in range(1, nsp):
            e = (me + d) % nsp
            send(remote(rs_out.at[e], rs_in.at[me], rs_s.at[0], rs_r.at[z], sp=e))
        rs_in[me] = rs_out[me]

    def row_scale(k):
        receive(rs_in.at[pl.ds(0, 2 if k else 1)], rs_r.at[chips[k]])
        return upright(rs_in[2 * chips[k]] + rs_in[2 * chips[k] + 1])[:, 0:1]

    depth = wg.shape[1]
    tile = min(256, depth)

    def expert_up(k):
        scale = row_scale(k)

        def up(n, carry):
            at = pl.ds(pl.multiple_of(n * tile, tile), tile)
            g = jnp.zeros((grp, tile), F32)
            u = jnp.zeros((grp, tile), F32)
            for b in range(ntp):
                x = arr[b, rows_of(k), :]
                g = g + dot(x, wg[b * ch:(b + 1) * ch, at])
                u = u + dot(x, wu[b * ch:(b + 1) * ch, at])
            hid[:, at] = (jax.nn.silu(g * scale) * (u * scale)).astype(BF16)
            return carry

        if k == 0:
            loads[1].wait()
            loads[2].wait()
        lax.fori_loop(0, depth // tile, up, 0)

    def down(k, b):
        at = pl.ds(pl.multiple_of(b * ch, ch), ch)
        part[b, rows_of(k), :] = dot(hid[...], wd[:, at]).astype(BF16)

    def down_far(k):
        if k == 0:
            loads[3].wait()
        down(k, td)
        if k > 0:
            first(k, 1, td, 0, tx)
            first(k, 3, td, 1, ty)

    def down_rest(k):
        down(k, tx)
        if k > 0:
            first(k, 0, tx, 0, tx)
        down(k, ty)
        if k > 0:
            first(k, 2, ty, 1, ty)
        down(k, t)

    def expert_down(k):
        down_far(k)
        down_rest(k)

    def sub(k, c, p):
        start = (2 * chips[k] + c) * cap + p * (cap // 2)
        return pl.ds(pl.multiple_of(start, cap // 2), cap // 2)

    def first(k, n, of, c, to):
        if n % 2:
            for p in range(2):
                send(remote(part.at[of, sub(k, c, p)], one.at[1, sub(k, c, p)], r_s.at[0],
                            r_r.at[8 * k + 2 * p + c], tp=to))
        else:
            send(remote(part.at[of, half(k, c)], one.at[0, half(k, c)], r_s.at[0],
                        r_r.at[8 * k + 4 + c], tp=to))

    def own_far(k):
        first(k, 1, td, 0, tx)
        first(k, 3, td, 1, ty)

    def own_near(k):
        first(k, 0, tx, 0, tx)
        first(k, 2, ty, 1, ty)

    def reduce_mid(k):
        for p in range(2):
            for c, to in ((0, ty), (1, tx)):
                at = sub(k, c, p)
                receive(one.at[1, at], r_r.at[8 * k + 2 * p + c])
                two_out[at, :] = (part[to, at, :].astype(F32) + one[1, at, :].astype(F32)).astype(
                    BF16
                )
                send(remote(two_out.at[at], two.at[at], r_s.at[0],
                            r_r.at[8 * k + 4 + 2 * p + c], tp=to))

    def reduce_end(k):
        for p in range(2):
            for c in range(2):
                at = sub(k, c, p)
                if p == 0:
                    receive(one.at[0, pl.ds(0, cap + cap // 2)], r_r.at[8 * k + 4 + c])
                else:
                    receive(two.at[at], r_r.at[8 * k + 6 + c])
                fin[at, :] = (
                    part[t, at, :].astype(F32) + one[0, at, :].astype(F32)
                    + two[at, :].astype(F32)
                ).astype(BF16)
                if k > 0:
                    back = pl.ds(pl.multiple_of(me * cap + p * (cap // 2), cap // 2), cap // 2)
                    send(remote(fin.at[at], ret.at[back], h_s.at[0], h_r.at[0],
                                sp=2 * chips[k] + c))
        if k == 0:
            send(remote(fin.at[piece(sib)], ret.at[piece(me)], h_s.at[0], h_r.at[0], sp=sib))
            ret[piece(me), :] = fin[piece(me), :]

    order = [
        (relay, 0), (share, 1), (gather_end, 0), (scales, 0), (place, 0), (share, 2), (relay, 1),
        (sibling, 0), (expert_up, 0), (expert_down, 0), (gather_end, 1), (relay, 2),
        (expert_up, 1), (expert_down, 1), (own_far, 0), (gather_end, 2),
        (expert_up, 2), (reduce_mid, 1), (expert_down, 2), (gather_end, 3), (expert_up, 3),
        (down_far, 3), (reduce_end, 1), (reduce_mid, 2), (down_rest, 3), (reduce_mid, 3),
        (own_near, 0), (reduce_mid, 0), (reduce_end, 2), (reduce_end, 3), (reduce_end, 0),
    ]
    for step, k in order:
        with jax.named_scope(step.__name__ + str(k)):
            step(k)

    with jax.named_scope("drain"):
        @pl.when(me < nsp - 1)
        def _():
            to_right.wait_send()

        @pl.when(me > 0)
        def _():
            to_left.wait_send()

        drain(lg_all.at[pl.ds(0, ntp - 1)], ln_s.at[0])
        drain(lb_all.at[pl.ds(0, ntp - 1)], ln_s.at[1])
        drain(rs_out.at[pl.ds(0, 2 * (ntp - 1))], st_s.at[0])
        drain(cc.at[pl.ds(0, 3)], ag_s.at[0])
        drain(outgoing.at[pl.ds(0, 4 * cap)], zs_s.at[0])
        drain(whole, zs_s.at[2])
        drain(near, zs_s.at[1])
        drain(rs_out.at[pl.ds(0, nsp - 1)], rs_s.at[0])
        drain(arr.at[pl.ds(0, 3), pl.ds(0, 6 * cap)], x_s.at[0])
        drain(arr.at[pl.ds(0, 3)], r_s.at[0])
    with jax.named_scope("ret"):
        receive(ret.at[pl.ds(0, (nsp - 1) * cap)], h_r.at[0])
    with jax.named_scope("final"):
        back = ret[...]
        moe = dot(pick0, back) * weights[:, 0:1] + dot(pick1, back) * weights[:, 1:2]
        out_ref[...] = (mixed[...] + moe).astype(out_ref.dtype)
        drain(ret.at[pl.ds(0, (nsp - 1) * cap)], h_s.at[0])


def fused(nsp, ntp, *args):
    (residual, glu_value, glu_gate, conv_weight, conv_bias, ln_gain, ln_bias, out_weight,
     norm_gain, route_ids, route_weight, expert_gate, expert_up, expert_down) = args
    rows, ch = residual.shape
    width = out_weight.shape[0]
    depth = expert_gate.shape[2]
    cap = 2 * rows * TOPK // nsp
    slots = nsp * cap
    grp = 2 * cap
    edge = -(-(conv_weight.shape[0] // 2) // 16) * 16
    small = [residual, glu_value, glu_gate, conv_weight]
    small += [a.reshape(1, ch) for a in (conv_bias, ln_gain, ln_bias, norm_gain)]
    small += [route_ids.T, route_weight.T]
    vmem = pl.BlockSpec(memory_space=pltpu.VMEM)
    hbm = pl.BlockSpec(memory_space=pl.ANY)
    dma = lambda n: pltpu.SemaphoreType.DMA((n,))
    return pl.pallas_call(
        functools.partial(layer_kernel, nsp, ntp),
        out_shape=jax.ShapeDtypeStruct((rows, ch), residual.dtype),
        in_specs=[hbm] * 14,
        out_specs=vmem,
        scratch_shapes=[pltpu.VMEM(a.shape, a.dtype) for a in small] + [
            pltpu.VMEM((width, ch), BF16),
            pltpu.VMEM((width, depth), BF16),
            pltpu.VMEM((width, depth), BF16),
            pltpu.VMEM((depth, width), BF16),
            pltpu.VMEM((rows + 2 * edge, ch), F32),
            pltpu.VMEM((-(-conv_weight.shape[0] // 8) * 8, ch), F32),
            pltpu.VMEM((rows, ch), F32),
            pltpu.VMEM((rows, ch), F32),
            pltpu.VMEM((2, edge, ch), BF16),
            pltpu.VMEM((2, edge, ch), BF16),
            pltpu.VMEM((2, 8, rows), F32),
            pltpu.VMEM((2, ntp, 8, rows), F32),
            pltpu.VMEM((ntp, 1, ch), F32),
            pltpu.VMEM((ntp, 1, ch), F32),
            pltpu.VMEM((ntp, rows, ch), BF16),
            pltpu.VMEM((slots, ch), BF16),
            pltpu.VMEM((ntp, slots, ch), BF16),
            pltpu.VMEM((grp, depth), BF16),
            pltpu.VMEM((ntp, slots, ch), BF16),
            pltpu.VMEM((2, slots, ch), BF16),
            pltpu.VMEM((slots, ch), BF16),
            pltpu.VMEM((slots, ch), BF16),
            pltpu.VMEM((slots, ch), BF16),
            pltpu.VMEM((slots, ch), BF16),
            pltpu.VMEM((nsp, 8, grp), F32),
            pltpu.VMEM((nsp, 8, grp), F32),
            pltpu.VMEM((ntp, rows, ch), BF16),
            pltpu.VMEM((slots, rows), BF16),
            pltpu.VMEM((ntp, cap, ch), BF16),
            pltpu.VMEM((2, ntp, cap, ch), BF16),
            pltpu.SemaphoreType.REGULAR((4,)), dma(14), dma(2), dma(2), dma(1), dma(2), dma(2), dma(2), dma(1), dma(7),
            dma(3), dma(nsp), dma(1), dma(GROUPS), dma(1), dma(5 * GROUPS - 5), dma(1),
            dma(8 * GROUPS), dma(1), dma(1),
        ],
        compiler_params=pltpu.CompilerParams(
            collective_id=0, has_side_effects=True, vmem_limit_bytes=VMEM_LIMIT
        ),
    )(*small, out_weight, expert_gate, expert_up, expert_down)


def solution(mesh):
    in_specs = (
        P("sp", "tp"),
        P("sp", "tp"),
        P("sp", "tp"),
        P(None, "tp"),
        P("tp"),
        P("tp"),
        P("tp"),
        P(None, "tp"),
        P("tp"),
        P("sp", None),
        P("sp", None),
        P("sp", None, "tp"),
        P("sp", None, "tp"),
        P("sp", "tp", None),
    )
    out_specs = P("sp", "tp")
    nsp, ntp = mesh.shape["sp"], mesh.shape["tp"]
    body = on_device
    if ntp == 4 and nsp == 2 * GROUPS:
        body = functools.partial(fused, nsp, ntp)
    return jax.shard_map(
        body, mesh=mesh, in_specs=in_specs, out_specs=out_specs, check_vma=False
    )
```

```python
import functools

import jax
import jax.numpy as jnp
from jax import lax
from jax.experimental import pallas as pl
from jax.experimental.pallas import tpu as pltpu
from jax.sharding import PartitionSpec as P

TOPK = 2


def with_halo(cells, sides, width):
    for axis, dim in sides:
        count = lax.axis_size(axis)
        ends = count - 1
        head = lax.slice_in_dim(cells, 0, width, axis=dim)
        tail = lax.slice_in_dim(cells, cells.shape[dim] - width, cells.shape[dim], axis=dim)
        cells = jnp.concatenate(
            [
                lax.ppermute(tail, axis, [(i, (i + 1) % count) for i in range(ends)]),
                cells,
                lax.ppermute(head, axis, [((i + 1) % count, i) for i in range(ends)]),
            ],
            axis=dim,
        )
    return cells


def on_device(
    residual,
    glu_value,
    glu_gate,
    conv_weight,
    conv_bias,
    ln_gain,
    ln_bias,
    out_weight,
    norm_gain,
    route_ids,
    route_weight,
    expert_gate,
    expert_up,
    expert_down,
):
    rows = residual.shape[0]
    width_all = out_weight.shape[0]
    gated = (glu_value.astype(jnp.float32) * jax.nn.sigmoid(glu_gate.astype(jnp.float32))).astype(
        jnp.bfloat16
    )
    reach = conv_weight.shape[0] // 2
    padded = with_halo(gated, (("sp", 0),), reach)
    taps = conv_weight.astype(jnp.float32)
    conv = jnp.zeros(gated.shape, jnp.float32) + conv_bias
    for tap in range(conv_weight.shape[0]):
        conv = conv + padded[tap : tap + rows].astype(jnp.float32) * taps[tap]
    totals = lax.psum((jnp.sum(conv, axis=1), jnp.sum(conv * conv, axis=1)), "tp")
    mean = (totals[0] / width_all)[:, None]
    var = (totals[1] / width_all)[:, None] - mean * mean
    act = jax.nn.silu((conv - mean) * lax.rsqrt(var + 1e-05) * ln_gain + ln_bias).astype(
        jnp.bfloat16
    )
    projected = jnp.dot(
        lax.all_gather(act, "tp", axis=1, tiled=True),
        out_weight,
        preferred_element_type=jnp.float32,
    )
    mixed = residual.astype(jnp.float32) + projected
    squares = lax.psum(jnp.sum(mixed * mixed, axis=1), "tp")
    normed = (mixed * lax.rsqrt(squares / width_all + 1e-06)[:, None] * norm_gain).astype(
        jnp.bfloat16
    )
    experts = lax.axis_size("sp")
    capacity = 2 * rows * TOPK // experts
    flat = route_ids.reshape(-1)
    onehot = (flat[:, None] == jnp.arange(experts, dtype=jnp.int32)[None, :]).astype(jnp.int32)
    rank = jnp.sum((jnp.cumsum(onehot, axis=0) - 1) * onehot, axis=1)
    slot_of = flat * capacity + rank
    placing = (slot_of[None, :] == jnp.arange(experts * capacity, dtype=jnp.int32)[:, None]).astype(
        jnp.bfloat16
    )
    copies = jnp.repeat(normed, TOPK, axis=0)
    outgoing = jnp.dot(placing, copies, preferred_element_type=jnp.float32).astype(jnp.bfloat16)
    outgoing = outgoing.reshape(experts, capacity, normed.shape[1])
    arrived = lax.all_to_all(outgoing, "sp", split_axis=0, concat_axis=0, tiled=True)
    arrived = lax.all_gather(
        arrived.reshape(experts * capacity, normed.shape[1]), "tp", axis=1, tiled=True
    )
    gate = jnp.dot(arrived, expert_gate[0], preferred_element_type=jnp.float32)
    up = jnp.dot(arrived, expert_up[0], preferred_element_type=jnp.float32)
    hidden = (jax.nn.silu(gate) * up).astype(jnp.bfloat16)
    partial_out = jnp.dot(hidden, expert_down[0], preferred_element_type=jnp.float32)
    summed = lax.psum_scatter(
        partial_out.astype(jnp.bfloat16), "tp", scatter_dimension=1, tiled=True
    )
    summed = summed.reshape(experts, capacity, summed.shape[1])
    returned = lax.all_to_all(summed, "sp", split_axis=0, concat_axis=0, tiled=True)
    returned = returned.reshape(experts * capacity, returned.shape[2])
    picked = lax.dot_general(
        placing, returned, (((0,), (0,)), ((), ())), preferred_element_type=jnp.float32
    )
    picked = picked.reshape(rows, TOPK, picked.shape[1])
    moe = jnp.sum(picked * route_weight[:, :, None], axis=1)
    return (mixed + moe).astype(jnp.bfloat16)


F32 = jnp.float32
BF16 = jnp.bfloat16
GROUPS = 4
VMEM_LIMIT = 67043328


def dot(a, b):
    return jnp.dot(a, b, preferred_element_type=F32)


def layer_kernel(
    nsp, ntp,
    res_hbm, val_hbm, gate_hbm, cw_hbm, cb_hbm, lg_hbm, lb_hbm, ng_hbm, ids_hbm, rw_hbm,
    ow_hbm, eg_hbm, eu_hbm, ed_hbm,
    out_ref,
    res_ref, val_ref, gate_ref, cw_ref, cb_ref, lg_ref, lb_ref, ng_ref, ids_ref, rw_ref,
    ow, wg, wu, wd, pad, wf, conv, mixed, halo_out, halo_in, st_out, st_in, lg_all, lb_all,
    cc, outgoing, arr, hid, part, one, two_out, two, fin, ret, rs_out, rs_in,
    tok, placed, near, whole,
    here, w_sem, halo_s, halo_r, st_s, st_r, ln_s, ln_r, ag_s, ag_r, zs_s, zs_r, rs_s, rs_r,
    x_s, x_r, r_s, r_r, h_s, h_r,
):
    rows, ch = res_ref.shape
    width = ow.shape[0]
    taps = cw_ref.shape[0]
    reach = taps // 2
    edge = halo_in.shape[1]
    cap = outgoing.shape[0] // nsp
    grp = 2 * cap
    last = GROUPS - 1
    me = lax.axis_index("sp")
    t = lax.axis_index("tp")
    z, mi = me // 2, me % 2
    cx, cy = t % 2, t // 2
    tx = cy * 2 + 1 - cx
    ty = (1 - cy) * 2 + cx
    td = (1 - cy) * 2 + 1 - cx
    far_side = z // 2
    inner = (z + far_side) % 2
    sign = 1 - 2 * far_side
    chips = [
        z,
        far_side * last + sign * last,
        far_side * last + sign * (1 + inner),
        far_side * last + sign * (2 - 2 * inner),
    ]
    sib = 2 * z + 1 - mi

    def remote(src, dst, ss, rs, **dev):
        return pltpu.make_async_remote_copy(
            src_ref=src, dst_ref=dst, send_sem=ss, recv_sem=rs,
            device_id=dev, device_id_type=pl.DeviceIdType.MESH,
        )

    smalls = [
        (val_hbm, val_ref), (gate_hbm, gate_ref), (cw_hbm, cw_ref), (cb_hbm, cb_ref),
        (lg_hbm, lg_ref), (lb_hbm, lb_ref), (ids_hbm, ids_ref), (res_hbm, res_ref),
        (ng_hbm, ng_ref), (rw_hbm, rw_ref),
    ]
    staged = [pltpu.make_async_copy(a, b, w_sem.at[4 + n]) for n, (a, b) in enumerate(smalls)]
    for load in staged:
        load.start()
    barrier = pltpu.get_barrier_semaphore()

    def signal(sem, **dev):
        pl.semaphore_signal(sem, inc=1, device_id=dev, device_id_type=pl.DeviceIdType.MESH)

    def along(d, act):
        pl.when(me >= d)(lambda: act(me - d))
        pl.when(me < nsp - d)(lambda: act(me + d))

    def present(d):
        return (me + nsp - d) // nsp + (2 * nsp - 1 - d - me) // nsp

    signal(barrier, tp=tx)
    signal(barrier, tp=ty)
    along(1, lambda e: signal(barrier, sp=e))
    loads = [
        pltpu.make_async_copy(ow_hbm, ow, w_sem.at[0]),
        pltpu.make_async_copy(eg_hbm.at[0], wg, w_sem.at[1]),
        pltpu.make_async_copy(eu_hbm.at[0], wu, w_sem.at[2]),
        pltpu.make_async_copy(ed_hbm.at[0], wd, w_sem.at[3]),
    ]
    for load in loads:
        load.start()

    with jax.named_scope("glu"):
        staged[0].wait()
        staged[1].wait()
        gated = (val_ref[...].astype(F32) * jax.nn.sigmoid(gate_ref[...].astype(F32))).astype(BF16)
        halo_out[0] = gated[rows - edge:]
        halo_out[1] = gated[:edge]
        pad[edge:edge + rows, :] = gated.astype(F32)
        pad[0:edge, :] = jnp.zeros((edge, ch), F32)
        pad[edge + rows:, :] = jnp.zeros((edge, ch), F32)
        for load in staged[2:6]:
            load.wait()
        wf[0:taps, :] = cw_ref[...].astype(F32)
    with jax.named_scope("bar"):
        pl.semaphore_wait(barrier, 2 + present(1))
    to_right = remote(halo_out.at[0], halo_in.at[0], halo_s.at[0], halo_r.at[0], sp=(me + 1) % nsp)
    to_left = remote(halo_out.at[1], halo_in.at[1], halo_s.at[1], halo_r.at[1],
                     sp=(me + nsp - 1) % nsp)

    @pl.when(me < nsp - 1)
    def _():
        to_right.start()

    @pl.when(me > 0)
    def _():
        to_left.start()

    def send(copy):
        copy.start()

    def drain(ref, sem):
        remote(ref, ref, sem, sem, tp=tx).wait_send()

    def receive(ref, sem):
        remote(ref, ref, sem, sem, tp=tx).wait_recv()

    others = (tx, ty, td)

    def send_ln(to):
        send(remote(lg_ref, lg_all.at[t], ln_s.at[0], ln_r.at[0], tp=to))
        send(remote(lb_ref, lb_all.at[t], ln_s.at[1], ln_r.at[1], tp=to))

    signal(here.at[0], tp=tx)
    along(1, lambda e: signal(here.at[1], sp=e))
    send_ln(tx)
    send_ln(ty)

    def heard(n):
        pl.semaphore_wait(here.at[1 + n // 2], present(n))
        if n < 4:
            along(2 * n, lambda e: signal(here.at[1 + n], sp=e))

    def convolve(low, high):
        for j in range(0, ch, 128):
            total = jnp.zeros((high - low, 128), F32) + cb_ref[:, j:j + 128]
            for tap in range(taps):
                at = low + tap + edge - reach
                total = total + pad[at:at + high - low, j:j + 128] * wf[tap:tap + 1, j:j + 128]
            conv[low:high, j:j + 128] = total

    with jax.named_scope("conv_mid"):
        convolve(edge, rows - edge)

    with jax.named_scope("halo"):
        pl.semaphore_wait(here.at[0], 1)
        send_ln(td)

        @pl.when(me > 0)
        def _():
            to_right.wait_recv()
            pad[0:edge, :] = halo_in[0].astype(F32)

        @pl.when(me < nsp - 1)
        def _():
            to_left.wait_recv()
            pad[edge + rows:, :] = halo_in[1].astype(F32)

        heard(1)

    with jax.named_scope("conv_edge"):
        convolve(0, edge)
        convolve(rows - edge, rows)

    lane = lax.broadcasted_iota(jnp.int32, (rows, 128), 1)

    def send_totals(which, sums):
        block = jnp.zeros((rows, 128), F32)
        for n, s in enumerate(sums):
            block = jnp.where(lane == n, s, block)
        st_out[which] = block.T[0:8, :]
        for to in others:
            send(remote(st_out.at[which], st_in.at[which, t], st_s.at[0], st_r.at[which], tp=to))

    def totals(which):
        receive(st_in.at[which, pl.ds(0, ntp - 1)], st_r.at[which])
        return [st_out[which]] + [st_in[which, b] for b in others]

    def upright(block):
        fill = jnp.zeros((128 - block.shape[0], block.shape[1]), F32)
        return jnp.concatenate([block, fill], axis=0).T

    quart = rows // 4

    def quarter(of, q):
        return cc.at[of, pl.ds(q * quart, quart)]

    with jax.named_scope("center"):
        c = conv[...]
        s1 = jnp.sum(c, axis=1, keepdims=True)
        c = c - s1 / ch
        cc[t] = c.astype(BF16)
        send_totals(0, (s1, jnp.sum(c * c, axis=1, keepdims=True)))
        for q in (0, 1, 2, 3):
            block = quarter(t, q)
            send(remote(block, block, ag_s.at[0], ag_r.at[q], tp=(tx, ty)[q % 2]))
        for q in (1, 0, 3, 2):
            block = quarter(t, q)
            send(remote(block, block, ag_s.at[0], ag_r.at[5 - q % 2], tp=(ty, tx)[q % 2]))

    with jax.named_scope("routes"):
        row = lax.broadcasted_iota(jnp.int32, (rows, rows), 0)
        col = lax.broadcasted_iota(jnp.int32, (rows, rows), 1)
        for load in staged[6:]:
            load.wait()
        ids = upright(ids_ref[...].astype(F32)).astype(jnp.int32)
        id0, id1 = ids[:, 0:1], ids[:, 1:2]
        weights = upright(rw_ref[...])
        hit0, hit1 = lane == id0, lane == id1
        named = jnp.where(hit0, 1.0, jnp.where(hit1, 1.0, 0.0)).astype(BF16)
        before = jnp.where(col < row, 1.0, 0.0).astype(BF16)
        rank = dot(before, named)
        rank0 = jnp.sum(jnp.where(hit0, rank, 0.0), axis=1, keepdims=True).astype(jnp.int32)
        rank1 = jnp.sum(jnp.where(hit1, rank, 0.0), axis=1, keepdims=True).astype(jnp.int32)
        slot = lax.broadcasted_iota(jnp.int32, (rows, nsp * cap), 1)
        pick0 = jnp.where(slot == id0 * cap + rank0, 1.0, 0.0)
        pick1 = jnp.where(slot == id1 * cap + rank1, 1.0, 0.0)
        placed[...] = (pick0 + pick1).T.astype(BF16)
        pick0 = pick0.astype(BF16)
        pick1 = pick1.astype(BF16)
        wide = lax.broadcasted_iota(jnp.int32, (rows, nsp * grp), 1)
        lead0, lead1 = id0 * grp + mi * cap + rank0, id1 * grp + mi * cap + rank1
        pick_r = jnp.where(wide == lead0, 1.0, jnp.where(wide == lead1, 1.0, 0.0)).astype(BF16)

    def relay_ag(q):
        of, to = ((tx, ty), (ty, tx))[q % 2]
        block = quarter(of, q)
        receive(block, ag_r.at[q])
        send(remote(block, block, ag_s.at[0], ag_r.at[6], tp=to))

    def columns(of):
        return ow[pl.ds(pl.multiple_of(of * ch, ch), ch), :]

    with jax.named_scope("relay_a"):
        relay_ag(0)
        relay_ag(1)
        heard(2)
    with jax.named_scope("relay_b"):
        relay_ag(2)
        relay_ag(3)
        receive(lg_all.at[pl.ds(0, ntp - 1)], ln_r.at[0])
        receive(lb_all.at[pl.ds(0, ntp - 1)], ln_r.at[1])
    with jax.named_scope("ln_stats"):
        lg_all[t] = lg_ref[...]
        lb_all[t] = lb_ref[...]
        stats = totals(0)
        total = stats[0] + stats[1] + stats[2] + stats[3]
        mean = total[0:1] / width
        offs = [s[0:1] / ch - mean for s in stats]
        spread = sum(o * o for o in offs)
        rstd = lax.rsqrt((total[1:2] + ch * spread) / width + 1e-05)
        cols = upright(jnp.concatenate([rstd] + [o * rstd for o in offs], axis=0))
        rstd = cols[:, 0:1]

    def project(of, n):
        a = cc[of].astype(F32) * rstd + cols[:, n:n + 1]
        a = jax.nn.silu(a * lg_all[of] + lb_all[of]).astype(BF16)
        return dot(a, columns(of))

    with jax.named_scope("proj_own"):
        loads[0].wait()
        mixed[...] = res_ref[...].astype(F32) + project(t, 1)
    with jax.named_scope("proj_x"):
        receive(cc.at[tx, pl.ds(0, 2 * quart)], ag_r.at[4])
        mixed[...] += project(tx, 2)
    with jax.named_scope("proj_y"):
        receive(cc.at[ty, pl.ds(0, 2 * quart)], ag_r.at[5])
        mixed[...] += project(ty, 3)
        heard(4)
    with jax.named_scope("proj_d"):
        receive(cc.at[td], ag_r.at[6])
        full = mixed[...] + project(td, 4)
        mixed[...] = full
    def piece(n):
        return pl.ds(pl.multiple_of(n * cap, cap), cap)

    def pass_on(k, n, block, to):
        send(remote(block, block, x_s.at[0], x_r.at[5 * k + n], tp=to))

    with jax.named_scope("pick"):
        tok[t] = (full * ng_ref[...]).astype(BF16)
        parts = [tok.at[t, pl.ds(q * quart, quart)] for q in range(4)]
        for q in range(4):
            pass_on(0, q, parts[q], (tx, ty)[q % 2])
        for q in range(4):
            pass_on(0, 4, parts[q ^ 1], (tx, ty)[q % 2])
        outgoing[...] = dot(placed[...], tok[t]).astype(BF16)

    def dispatch(e):
        remote(outgoing.at[piece(e)], arr.at[t, piece(me)], zs_s.at[0], zs_r.at[me], sp=e).start()

    def dispatch_chip(c):
        dispatch(2 * c + mi)
        dispatch(2 * c + 1 - mi)

    last_chip = far_side * last + sign * (1 + 2 * inner)
    with jax.named_scope("zsend"):
        dispatch_chip(far_side * last + sign * (3 - 3 * inner))
        dispatch_chip(far_side * last + sign * 2)

        send_totals(1, (jnp.sum(full * full, axis=1, keepdims=True),))

    def rows_of(k):
        return pl.ds(pl.multiple_of(chips[k] * grp, grp), grp)

    def half(k, c):
        return piece(2 * chips[k] + c)

    def way(k, of, q):
        if k == 0:
            return tok.at[of, pl.ds(q * quart, quart)]
        start = 2 * chips[k] * cap + q * (cap // 2)
        return arr.at[of, pl.ds(pl.multiple_of(start, cap // 2), cap // 2)]

    def share(k, cores=(1, 0)):
        for c in cores:
            e = 2 * chips[k] + c
            receive(arr.at[t, piece(e)], zs_r.at[e])
            one_way, other = way(k, t, 2 * c), way(k, t, 2 * c + 1)
            pass_on(k, 2 * c, one_way, tx)
            pass_on(k, 2 * c + 1, other, ty)
            pass_on(k, 4, other, tx)
            pass_on(k, 4, one_way, ty)

    def share_one(k):
        share(k, (1,))

    def share_zero(k):
        share(k, (0,))

    def relay(k):
        for q in (2, 3, 0, 1) if k else (0, 1, 2, 3):
            of, to = ((tx, ty), (ty, tx))[q % 2]
            receive(way(k, of, q), x_r.at[5 * k + q])
            pass_on(k, 4, way(k, of, q), to)

    def gather_end(k):
        if k < last:
            receive(arr.at[0, pl.ds(0, 4 * cap)], x_r.at[5 * k + 4])
            return
        for c in (1, 0):
            e = 2 * chips[k] + c
            receive(arr.at[:, piece(e)], zs_r.at[e])

    def place(k):
        to = [me, sib, 2 * last_chip, 2 * last_chip + 1]
        both = jnp.concatenate([placed[piece(e), :] for e in to], axis=0)
        for b in range(ntp):
            rows_b = dot(both, tok[b]).astype(BF16)
            arr[b, piece(me), :] = rows_b[:cap]
            near[b] = rows_b[cap:2 * cap]
            whole[0, b] = rows_b[2 * cap:3 * cap]
            whole[1, b] = rows_b[3 * cap:]
        send(remote(near, arr.at[:, piece(me)], zs_s.at[1], zs_r.at[me], sp=sib))
        for c in (0, 1):
            send(remote(whole.at[c], arr.at[:, piece(me)], zs_s.at[2], zs_r.at[me], sp=to[2 + c]))

    def sibling(k):
        receive(arr.at[:, piece(sib)], zs_r.at[sib])

    def scales(k):
        r = lax.rsqrt(sum(totals(1)) / width + 1e-06)[0:1]
        top = r.astype(BF16).astype(F32)
        mid = (r - top).astype(BF16).astype(F32)
        low = r - top - mid
        three = jnp.concatenate([top, mid, low, jnp.zeros((13, rows), F32)], axis=0).astype(BF16)
        picked = dot(three, pick_r)
        picked = picked[0:1] + picked[1:2] + picked[2:3]
        for e in range(nsp):
            rs_out[e] = jnp.broadcast_to(picked[:, e * grp:(e + 1) * grp], (8, grp))
        for d in range(1, nsp):
            e = (me + d) % nsp
            send(remote(rs_out.at[e], rs_in.at[me], rs_s.at[0], rs_r.at[z], sp=e))
        rs_in[me] = rs_out[me]

    def row_scale(k):
        receive(rs_in.at[pl.ds(0, 2 if k else 1)], rs_r.at[chips[k]])
        return upright(rs_in[2 * chips[k]] + rs_in[2 * chips[k] + 1])[:, 0:1]

    depth = wg.shape[1]
    tile = min(256, depth)

    def expert_up(k):
        scale = row_scale(k)

        def up(n, carry):
            at = pl.ds(pl.multiple_of(n * tile, tile), tile)
            g = jnp.zeros((grp, tile), F32)
            u = jnp.zeros((grp, tile), F32)
            for b in range(ntp):
                x = arr[b, rows_of(k), :]
                g = g + dot(x, wg[b * ch:(b + 1) * ch, at])
                u = u + dot(x, wu[b * ch:(b + 1) * ch, at])
            hid[:, at] = (jax.nn.silu(g * scale) * (u * scale)).astype(BF16)
            return carry

        if k == 0:
            loads[1].wait()
            loads[2].wait()
        lax.fori_loop(0, depth // tile, up, 0)

    def down(k, b):
        at = pl.ds(pl.multiple_of(b * ch, ch), ch)
        part[b, rows_of(k), :] = dot(hid[...], wd[:, at]).astype(BF16)

    def down_far(k):
        if k == 0:
            loads[3].wait()
        down(k, td)
        if k > 0:
            first(k, 1, td, 0, tx)
            first(k, 3, td, 1, ty)

    def down_rest(k):
        down(k, tx)
        if k > 0:
            first(k, 0, tx, 0, tx)
        down(k, ty)
        if k > 0:
            first(k, 2, ty, 1, ty)
        down(k, t)

    def expert_down(k):
        down_far(k)
        down_rest(k)

    def sub(k, c, p):
        start = (2 * chips[k] + c) * cap + p * (cap // 2)
        return pl.ds(pl.multiple_of(start, cap // 2), cap // 2)

    def first(k, n, of, c, to):
        if n % 2:
            for p in range(2):
                send(remote(part.at[of, sub(k, c, p)], one.at[1, sub(k, c, p)], r_s.at[0],
                            r_r.at[8 * k + 2 * p + c], tp=to))
        else:
            send(remote(part.at[of, half(k, c)], one.at[0, half(k, c)], r_s.at[0],
                        r_r.at[8 * k + 4 + c], tp=to))

    def own_far(k):
        first(k, 1, td, 0, tx)
        first(k, 3, td, 1, ty)

    def own_near(k):
        first(k, 0, tx, 0, tx)
        first(k, 2, ty, 1, ty)

    def reduce_mid(k):
        for p in range(2):
            for c, to in ((0, ty), (1, tx)):
                at = sub(k, c, p)
                receive(one.at[1, at], r_r.at[8 * k + 2 * p + c])
                two_out[at, :] = (part[to, at, :].astype(F32) + one[1, at, :].astype(F32)).astype(
                    BF16
                )
                send(remote(two_out.at[at], two.at[at], r_s.at[0],
                            r_r.at[8 * k + 4 + 2 * p + c], tp=to))

    def reduce_end(k):
        for p in range(2):
            for c in range(2):
                at = sub(k, c, p)
                if p == 0:
                    receive(one.at[0, pl.ds(0, cap + cap // 2)], r_r.at[8 * k + 4 + c])
                else:
                    receive(two.at[at], r_r.at[8 * k + 6 + c])
                fin[at, :] = (
                    part[t, at, :].astype(F32) + one[0, at, :].astype(F32)
                    + two[at, :].astype(F32)
                ).astype(BF16)
                if k > 0:
                    back = pl.ds(pl.multiple_of(me * cap + p * (cap // 2), cap // 2), cap // 2)
                    send(remote(fin.at[at], ret.at[back], h_s.at[0], h_r.at[0],
                                sp=2 * chips[k] + c))
        if k == 0:
            send(remote(fin.at[piece(sib)], ret.at[piece(me)], h_s.at[0], h_r.at[0], sp=sib))
            ret[piece(me), :] = fin[piece(me), :]

    order = [
        (relay, 0), (share, 1), (gather_end, 0), (scales, 0), (place, 0), (share_one, 2), (relay, 1), (share_zero, 2),
        (sibling, 0), (expert_up, 0), (expert_down, 0), (gather_end, 1), (relay, 2),
        (expert_up, 1), (expert_down, 1), (own_far, 0), (gather_end, 2),
        (expert_up, 2), (reduce_mid, 1), (expert_down, 2), (gather_end, 3), (expert_up, 3),
        (down_far, 3), (reduce_end, 1), (reduce_mid, 2), (down_rest, 3), (reduce_mid, 3),
        (own_near, 0), (reduce_mid, 0), (reduce_end, 2), (reduce_end, 3), (reduce_end, 0),
    ]
    for step, k in order:
        with jax.named_scope(step.__name__ + str(k)):
            step(k)

    with jax.named_scope("drain"):
        @pl.when(me < nsp - 1)
        def _():
            to_right.wait_send()

        @pl.when(me > 0)
        def _():
            to_left.wait_send()

        drain(lg_all.at[pl.ds(0, ntp - 1)], ln_s.at[0])
        drain(lb_all.at[pl.ds(0, ntp - 1)], ln_s.at[1])
        drain(rs_out.at[pl.ds(0, 2 * (ntp - 1))], st_s.at[0])
        drain(cc.at[pl.ds(0, 3)], ag_s.at[0])
        drain(outgoing.at[pl.ds(0, 4 * cap)], zs_s.at[0])
        drain(whole, zs_s.at[2])
        drain(near, zs_s.at[1])
        drain(rs_out.at[pl.ds(0, nsp - 1)], rs_s.at[0])
        drain(arr.at[pl.ds(0, 3), pl.ds(0, 6 * cap)], x_s.at[0])
        drain(arr.at[pl.ds(0, 3)], r_s.at[0])
    with jax.named_scope("ret"):
        receive(ret.at[pl.ds(0, (nsp - 1) * cap)], h_r.at[0])
    with jax.named_scope("final"):
        back = ret[...]
        moe = dot(pick0, back) * weights[:, 0:1] + dot(pick1, back) * weights[:, 1:2]
        out_ref[...] = (mixed[...] + moe).astype(out_ref.dtype)
        drain(ret.at[pl.ds(0, (nsp - 1) * cap)], h_s.at[0])


def fused(nsp, ntp, *args):
    (residual, glu_value, glu_gate, conv_weight, conv_bias, ln_gain, ln_bias, out_weight,
     norm_gain, route_ids, route_weight, expert_gate, expert_up, expert_down) = args
    rows, ch = residual.shape
    width = out_weight.shape[0]
    depth = expert_gate.shape[2]
    cap = 2 * rows * TOPK // nsp
    slots = nsp * cap
    grp = 2 * cap
    edge = -(-(conv_weight.shape[0] // 2) // 16) * 16
    small = [residual, glu_value, glu_gate, conv_weight]
    small += [a.reshape(1, ch) for a in (conv_bias, ln_gain, ln_bias, norm_gain)]
    small += [route_ids.T, route_weight.T]
    vmem = pl.BlockSpec(memory_space=pltpu.VMEM)
    hbm = pl.BlockSpec(memory_space=pl.ANY)
    dma = lambda n: pltpu.SemaphoreType.DMA((n,))
    return pl.pallas_call(
        functools.partial(layer_kernel, nsp, ntp),
        out_shape=jax.ShapeDtypeStruct((rows, ch), residual.dtype),
        in_specs=[hbm] * 14,
        out_specs=vmem,
        scratch_shapes=[pltpu.VMEM(a.shape, a.dtype) for a in small] + [
            pltpu.VMEM((width, ch), BF16),
            pltpu.VMEM((width, depth), BF16),
            pltpu.VMEM((width, depth), BF16),
            pltpu.VMEM((depth, width), BF16),
            pltpu.VMEM((rows + 2 * edge, ch), F32),
            pltpu.VMEM((-(-conv_weight.shape[0] // 8) * 8, ch), F32),
            pltpu.VMEM((rows, ch), F32),
            pltpu.VMEM((rows, ch), F32),
            pltpu.VMEM((2, edge, ch), BF16),
            pltpu.VMEM((2, edge, ch), BF16),
            pltpu.VMEM((2, 8, rows), F32),
            pltpu.VMEM((2, ntp, 8, rows), F32),
            pltpu.VMEM((ntp, 1, ch), F32),
            pltpu.VMEM((ntp, 1, ch), F32),
            pltpu.VMEM((ntp, rows, ch), BF16),
            pltpu.VMEM((slots, ch), BF16),
            pltpu.VMEM((ntp, slots, ch), BF16),
            pltpu.VMEM((grp, depth), BF16),
            pltpu.VMEM((ntp, slots, ch), BF16),
            pltpu.VMEM((2, slots, ch), BF16),
            pltpu.VMEM((slots, ch), BF16),
            pltpu.VMEM((slots, ch), BF16),
            pltpu.VMEM((slots, ch), BF16),
            pltpu.VMEM((slots, ch), BF16),
            pltpu.VMEM((nsp, 8, grp), F32),
            pltpu.VMEM((nsp, 8, grp), F32),
            pltpu.VMEM((ntp, rows, ch), BF16),
            pltpu.VMEM((slots, rows), BF16),
            pltpu.VMEM((ntp, cap, ch), BF16),
            pltpu.VMEM((2, ntp, cap, ch), BF16),
            pltpu.SemaphoreType.REGULAR((4,)), dma(14), dma(2), dma(2), dma(1), dma(2), dma(2), dma(2), dma(1), dma(7),
            dma(3), dma(nsp), dma(1), dma(GROUPS), dma(1), dma(5 * GROUPS - 5), dma(1),
            dma(8 * GROUPS), dma(1), dma(1),
        ],
        compiler_params=pltpu.CompilerParams(
            collective_id=0, has_side_effects=True, vmem_limit_bytes=VMEM_LIMIT
        ),
    )(*small, out_weight, expert_gate, expert_up, expert_down)


def solution(mesh):
    in_specs = (
        P("sp", "tp"),
        P("sp", "tp"),
        P("sp", "tp"),
        P(None, "tp"),
        P("tp"),
        P("tp"),
        P("tp"),
        P(None, "tp"),
        P("tp"),
        P("sp", None),
        P("sp", None),
        P("sp", None, "tp"),
        P("sp", None, "tp"),
        P("sp", "tp", None),
    )
    out_specs = P("sp", "tp")
    nsp, ntp = mesh.shape["sp"], mesh.shape["tp"]
    body = on_device
    if ntp == 4 and nsp == 2 * GROUPS:
        body = functools.partial(fused, nsp, ntp)
    return jax.shard_map(
        body, mesh=mesh, in_specs=in_specs, out_specs=out_specs, check_vma=False
    )
```
